32 devices in a mesh: ep: 8 (over z, core), tp: 4 (over y, x).
Axes of the slice: x: 2, y: 2, z: 4, core: 2. Of those that a mesh axis runs over, the one named last changes fastest.
Arguments:
- tokens: bfloat16 [1536, 4096], P('ep'), may hold values from -6 to 6
- expert_ids: int32 [1536, 2], P('ep'), may hold values from 0 to 7, all different within a row; in each aligned block of 192 rows (0 to 191, 192 to 383, ...) at most 60 rows name the same one
- route_weight: float32 [1536, 2], P('ep'), may hold values from 0.1 to 1
- norm_gain: float32 [4096], replicated, may hold values from 0.1 to 1.9
- gate_weight: bfloat16 [8, 4096, 4096], P('ep', None, 'tp'), may hold values from -0.28125 to 0.28125
- up_weight: bfloat16 [8, 4096, 4096], P('ep', None, 'tp'), may hold values from -0.28125 to 0.28125
- down_weight: bfloat16 [8, 4096, 4096], P('ep', None, 'tp'), may hold values from -0.028076172 to 0.028076172
Outputs:
- mixed: bfloat16 [1536, 4096], P('ep', 'tp')
The draws below stay inside these ranges and needn't reach their ends.
Inputs may be any that keep to these rules, and one draw needn't show every extreme that they name: `expert_ids`: each row names 2 different experts. In each aligned block of 192 rows (the tokens of one index of ep) no expert is named by more than 60 rows, and in some block some expert is named by exactly 60 rows.
All inputs are finite; a program needn't handle non-finite values.
Results may differ from the reference program's by a relative error of at most 0.007.
Values may be sent and summed in bfloat16 or wider, within the bound.
A program may use at most 64 MiB of HBM per device.

```python
import math
import jax
import jax.numpy as jnp
import numpy as np
from jax import lax

D = 4096
FF = 4096
TOPK = 2
TOK_EP = 192
EXPERTS = 8
TOKENS = 1536
CAP = 60
N_EP = 8


def block_scale(key, extent, pieces, least, top_value):
    level, own = 1.0, jax.random.fold_in(key, 6)
    for axis_at, parts in pieces:
        draws = jnp.exp(jax.random.uniform(jax.random.fold_in(own, axis_at), (parts,), jnp.float32, least / len(pieces), top_value / len(pieces)))
        level = level * jnp.repeat(draws, extent[axis_at] // parts).reshape([-1 if axis == axis_at else 1 for axis in range(len(extent))])
    return level


def shared_out(stream_key, own, number, rows, number_of, top, bound, skew):
    ranking = jax.random.permutation(stream_key, number_of)
    heavy_load, usual = load_shares(number_of, rows * top, bound, skew, True), load_shares(number_of, rows * top, bound, skew, False)
    places = jnp.arange(number_of)

    def named(lengths, turn):
        used = int((lengths > 0).sum())
        fixed = max(1, used // 4)
        shifted = fixed + (places - fixed + turn * (used - fixed)) % max(1, number_of - fixed)
        return jnp.zeros((number_of,), jnp.int32).at[ranking[jnp.where(places < fixed, places, shifted)]].set(jnp.asarray(lengths, jnp.int32))

    lengths = jnp.where(number % 4 == 0, named(heavy_load, number // 4), named(usual, number - number // 4 - 1))
    mixed = jax.random.permutation(jax.random.fold_in(own, 3), number_of)
    source_of, receiver = mixed[0:number_of // 2 * 2:2], mixed[1:number_of // 2 * 2:2]
    margin = jnp.minimum(lengths[source_of] - 1, bound - lengths[receiver]) // 2
    margin = jnp.where((source_of == ranking[0]) | (receiver == ranking[0]) | (lengths[receiver] == 0), 0, jnp.maximum(margin, 0))
    shifted = jax.random.randint(jax.random.fold_in(own, 4), (number_of // 2,), 0, 1 << 20) % (margin + 1)
    lengths = lengths.at[source_of].add(-shifted).at[receiver].add(shifted)
    items = jnp.searchsorted(jnp.cumsum(lengths), jnp.arange(rows * top), side="right").astype(jnp.int32)
    listing = items.reshape(top, rows).T
    listing = listing[jax.random.permutation(jax.random.fold_in(own, 1), rows)]
    turn = jax.random.randint(jax.random.fold_in(own, 2), (rows, 1), 0, top)
    return jnp.take_along_axis(listing, (jnp.arange(top)[None, :] + turn) % top, axis=1)


def load_shares(count, total, bound, slope, full):
    weights = [(1 << 20) // math.isqrt(standing ** slope) + 1 for standing in range(1, count + 1)]
    largest = bound if full else min(bound, max(-(-total // count), total * weights[0] // sum(weights)))
    least = 1 if total - largest >= count - 1 else 0
    counts, rest = [largest] + [least] * (count - 1), total - largest - least * (count - 1)
    while rest > 0:
        candidates = [i for i in range(1, count) if counts[i] < largest] or [i for i in range(1, count) if counts[i] < bound]
        whole, left = sum([weights[i] for i in candidates]), rest
        for i in candidates:
            extra = min(bound - counts[i], max(1, left * weights[i] // whole), rest)
            counts[i] = counts[i] + extra
            rest = rest - extra
    return np.array(counts)


def scatter_about(stream_key, dims, deviation, bound, cuts=(), kind=jnp.bfloat16):
    gain = block_scale(stream_key, dims, cuts, -0.22, 0.18) if cuts else 1.0
    entries = jax.random.normal(stream_key, dims, jnp.float32) * deviation * gain
    return jnp.minimum(jnp.maximum(entries, -bound), bound).astype(kind)


def setup_inputs(seed: int = 0) -> dict:
    keys = jax.random.split(jax.random.key(seed), 8)
    tokens = scatter_about(keys[0], (TOKENS, D), 1.0, 6.0, ((0, 8),))
    expert_ids_keys = jax.random.split(jax.random.fold_in(keys[1], 1), TOKENS // TOK_EP)
    expert_ids_turns = jax.random.permutation(jax.random.fold_in(keys[1], 3), TOKENS // TOK_EP)
    expert_ids = jax.vmap(lambda own, number: shared_out(jax.random.fold_in(keys[1], 2), own, number, TOK_EP, EXPERTS, TOPK, CAP, 2))(expert_ids_keys, expert_ids_turns).reshape((TOKENS, TOPK))
    route_weight = jnp.clip(0.1 + 0.9 * jax.random.uniform(keys[2], (TOKENS, TOPK), jnp.float32) ** block_scale(keys[2], (TOKENS, TOPK), ((0, 8),), -0.2, 0.2), 0.1, 1.0)
    norm_gain = jnp.clip(1.0 + 0.18 * jax.random.normal(keys[3], (D,), jnp.float32), 0.1, 1.9)
    gate_weight = scatter_about(keys[4], (EXPERTS, D, FF), (3.0 / D ** 0.5), 0.28125, ((0, 8), (2, 4)))
    up_weight = scatter_about(keys[5], (EXPERTS, D, FF), (3.0 / D ** 0.5), 0.28125, ((0, 8), (2, 4)))
    down_weight = scatter_about(keys[6], (EXPERTS, FF, D), (0.3 / FF ** 0.5), 0.028076172, ((0, 8), (2, 4)))
    return {"tokens": tokens, "expert_ids": expert_ids, "route_weight": route_weight, "norm_gain": norm_gain, "gate_weight": gate_weight, "up_weight": up_weight, "down_weight": down_weight}


EPS = 1e-06
LIMIT = 7.0
ALPHA = 1.702

def rms_norm(tokens, norm_gain):
    values = tokens.astype(jnp.float32)
    scale = lax.rsqrt(lax.optimization_barrier(jnp.mean(values * values, axis=-1, keepdims=True)) + EPS)
    return (values * scale * norm_gain.astype(jnp.float32)).astype(jnp.bfloat16)

def clamped_unit(gate_pre, up_pre):
    gate = jnp.minimum(gate_pre, LIMIT)
    up_part = jnp.clip(up_pre, -LIMIT, LIMIT)
    return ((up_part + 1.0) * gate * jax.nn.sigmoid(ALPHA * gate)).astype(jnp.bfloat16)

def reference(tokens, expert_ids, route_weight, norm_gain, gate_weight, up_weight, down_weight):
    normed = rms_norm(tokens, norm_gain)
    copies = TOK_EP * TOPK
    ids_blocks = expert_ids.reshape(N_EP, copies).astype(jnp.int32)
    onehot = (ids_blocks[:, :, None] == jnp.arange(EXPERTS, dtype=jnp.int32)[None, None, :]).astype(jnp.int32)
    before = jnp.cumsum(onehot, axis=1) - onehot
    position = lax.optimization_barrier(jnp.sum(before * onehot, axis=2)).astype(jnp.int32)
    block_ids = jnp.broadcast_to(jnp.arange(N_EP, dtype=jnp.int32)[:, None], (N_EP, copies))
    copy_token = (block_ids * TOK_EP + jnp.arange(copies, dtype=jnp.int32)[None, :] // TOPK).astype(jnp.int32)
    table = jnp.full((EXPERTS, N_EP, CAP), TOKENS, jnp.int32)
    table = table.at[ids_blocks, block_ids, position].set(copy_token)
    weight_table = jnp.zeros((EXPERTS, N_EP, CAP), jnp.float32)
    weight_table = weight_table.at[ids_blocks, block_ids, position].set(route_weight.reshape(N_EP, copies).astype(jnp.float32))
    padded = jnp.concatenate([normed, jnp.zeros((1, D), jnp.bfloat16)], axis=0)

    def one_expert(operands):
        gate_w, up_w, down_w, row_index, weights = operands
        rows = padded[row_index.reshape(-1)]
        gate_pre = jnp.dot(rows, gate_w, preferred_element_type=jnp.float32)
        up_pre = jnp.dot(rows, up_w, preferred_element_type=jnp.float32)
        hidden = clamped_unit(gate_pre, up_pre)
        result = jnp.dot(hidden, down_w, preferred_element_type=jnp.float32).astype(jnp.bfloat16)
        result = lax.optimization_barrier(result).astype(jnp.float32)
        return result * weights.reshape(-1)[:, None]
    outputs = lax.map(one_expert, (gate_weight, up_weight, down_weight, table, weight_table))
    total = jnp.zeros((TOKENS + 1, D), jnp.float32)
    total = total.at[table.reshape(-1)].add(outputs.reshape(-1, D))
    return total[:TOKENS].astype(jnp.bfloat16)
```

```python
import functools

import jax
import jax.numpy as jnp
from jax import lax
from jax.experimental import pallas as pl
from jax.experimental.pallas import tpu as pltpu
from jax.sharding import PartitionSpec as P

EPS = 1e-06
LIMIT = 7.0
ALPHA = 1.702


def rms_norm(tokens, norm_gain):
    values = tokens.astype(jnp.float32)
    scale = lax.rsqrt(jnp.mean(values * values, axis=-1, keepdims=True) + EPS)
    return (values * scale * norm_gain).astype(jnp.bfloat16)


def clamped_unit(gate_pre, up_pre):
    gate = jnp.minimum(gate_pre, LIMIT)
    up_part = jnp.clip(up_pre, -LIMIT, LIMIT)
    return ((up_part + 1.0) * gate * jax.nn.sigmoid(ALPHA * gate)).astype(jnp.bfloat16)


def slot_numbers(id_blocks, experts, capacity):
    onehot = (id_blocks[:, :, None] == jnp.arange(experts, dtype=jnp.int32)[None, None, :]).astype(
        jnp.int32
    )
    before = jnp.cumsum(onehot, axis=1) - onehot
    position = jnp.sum(before * onehot, axis=2)
    return id_blocks * capacity + position


def project_down(hidden, down_weight):
    result = jnp.einsum(
        "sejf,efd->sejd",
        lax.all_gather(hidden, "tp", axis=3, tiled=True),
        down_weight,
        preferred_element_type=jnp.float32,
    )
    return result.astype(jnp.bfloat16)


def plain_path(tokens, expert_ids, route_weight, norm_gain, gate_weight, up_weight, down_weight):
    n_ep = lax.axis_size("ep")
    n_tp = lax.axis_size("tp")
    tok_rows, width = tokens.shape
    top = expert_ids.shape[1]
    local_experts = gate_weight.shape[0]
    experts = local_experts * n_ep
    capacity = 5 * tok_rows * top // (4 * experts)
    cols = width // n_tp
    normed = rms_norm(tokens, norm_gain)
    dest = slot_numbers(expert_ids.reshape(1, tok_rows * top), experts, capacity).reshape(-1)
    slot_range = jnp.arange(experts * capacity, dtype=jnp.int32)
    match = slot_range[:, None] == dest[None, :]
    pick = jnp.any(match.reshape(experts * capacity, tok_rows, top), axis=2).astype(jnp.bfloat16)
    own = lax.dynamic_slice_in_dim(normed, lax.axis_index("tp") * cols, cols, 1)
    buffer = jnp.dot(pick, own, preferred_element_type=jnp.float32).astype(jnp.bfloat16)
    buffer = buffer.reshape(n_ep, local_experts, capacity, cols)
    arrived = lax.all_to_all(buffer, "ep", split_axis=0, concat_axis=0, tiled=True)
    piece = lax.all_gather(arrived, "tp", axis=3, tiled=True)
    gate_part = jnp.einsum("sejd,edf->sejf", piece, gate_weight, preferred_element_type=jnp.float32)
    up_part = jnp.einsum("sejd,edf->sejf", piece, up_weight, preferred_element_type=jnp.float32)
    hidden = clamped_unit(gate_part, up_part)
    result = project_down(hidden, down_weight)
    back = lax.all_to_all(result, "ep", split_axis=0, concat_axis=0, tiled=True).reshape(
        experts * capacity, cols
    )
    chosen = jnp.transpose(match).astype(jnp.bfloat16)
    per_copy = jnp.dot(chosen, back, preferred_element_type=jnp.float32).reshape(
        tok_rows, top, cols
    )
    mixed = jnp.sum(per_copy * route_weight[:, :, None], axis=1)
    return mixed.astype(jnp.bfloat16)


VMEM_BYTES = 47 * 1024 * 1024
COLUMN_TILE = 256
PIECES = 2


def flip(value, bits):
    bit = 1
    while bit <= bits:
        if bits & bit:
            value = value + bit - 2 * bit * lax.rem(lax.div(value, jnp.int32(bit)), jnp.int32(2))
        bit *= 2
    return value


def fused_kernel(
    n_ep,
    n_tp,
    capacity,
    slots,
    tokens_hbm,
    ids_row_hbm,
    route_row_hbm,
    gain_hbm,
    gate_hbm,
    up_hbm,
    down_hbm,
    out_ref,
    tokens_ref,
    ids_row_ref,
    route_row_ref,
    gain_ref,
    gate_v,
    up_v,
    down_v,
    scales,
    normed,
    outbox,
    fullbox,
    zbox,
    zfull,
    xbuf,
    hbuf,
    obuf,
    back,
    acc,
    small_sem,
    weight_sem,
    z_send,
    z_recv,
    pair_send,
    pair_recv,
    g_send,
    g_recv,
    b_send,
    b_recv,
):
    pairs = n_ep // 2
    rows = 2 * capacity
    lead = slots - capacity
    second = rows - slots
    tok_rows, width = tokens_ref.shape
    cols = xbuf.shape[-1]
    hid = hbuf.shape[-1]
    outs = obuf.shape[-1]
    ep = lax.axis_index("ep")
    tp = lax.axis_index("tp")
    pair = lax.div(ep, jnp.int32(2))
    core = lax.rem(ep, jnp.int32(2))
    side = (flip(tp, 1), flip(tp, 2))
    far = flip(tp, 3)
    upper = lax.div(pair, jnp.int32(2))
    inner = lax.rem(pair + upper, jnp.int32(2))
    early, late = 2 + inner, 3 - inner
    chip_of = {0: pair, 1: flip(pair, 1), "early": 2 - upper, "late": 3 - 3 * upper}
    slot_of = {0: 0, 1: 1, "early": early, "late": late}

    small = (
        (tokens_hbm, tokens_ref),
        (ids_row_hbm, ids_row_ref),
        (route_row_hbm, route_row_ref),
        (gain_hbm, gain_ref),
    )
    small_loads = [
        pltpu.make_async_copy(a, b, small_sem.at[i]) for i, (a, b) in enumerate(small)
    ]
    for load in small_loads:
        load.start()
    loads = [
        pltpu.make_async_copy(hbm.at[0], vmem, weight_sem.at[i])
        for i, (hbm, vmem) in enumerate(((gate_hbm, gate_v), (up_hbm, up_v), (down_hbm, down_v)))
    ]

    barrier = pltpu.get_barrier_semaphore()
    for k in range(1, n_ep):
        pl.semaphore_signal(
            barrier, inc=1, device_id=(flip(ep, k), tp), device_id_type=pl.DeviceIdType.MESH
        )
    for other in side:
        pl.semaphore_signal(
            barrier, inc=1, device_id=(ep, other), device_id_type=pl.DeviceIdType.MESH
        )

    with jax.named_scope("small_wait"):
        for load in small_loads:
            load.wait()
    for load in loads:
        load.start()

    own_cols = pl.ds(pl.multiple_of(tp * cols, cols), cols)
    far_cols = pl.ds(pl.multiple_of(far * cols, cols), cols)

    def scale_rows(i, carry):
        at = pl.ds(pl.multiple_of(i * 32, 32), 32)
        values = tokens_ref[at, :].astype(jnp.float32)
        scale = lax.rsqrt(jnp.mean(values * values, axis=-1, keepdims=True) + EPS)
        scales[at, :] = jnp.broadcast_to(scale, (32, scales.shape[1]))
        for where in (own_cols, far_cols):
            values = tokens_ref[at, where].astype(jnp.float32)
            normed[at, where] = (values * scale * gain_ref[:, where]).astype(jnp.bfloat16)
        return carry

    with jax.named_scope("scale_rows"):
        lax.fori_loop(0, tok_rows // 32, scale_rows, 0)

    ids_row = ids_row_ref[...]
    expert_col = lax.broadcasted_iota(jnp.int32, (n_ep, tok_rows), 0)
    hits_row = ((ids_row[0:1, :] == expert_col) | (ids_row[1:2, :] == expert_col)).astype(
        jnp.float32
    ).astype(jnp.bfloat16)
    first = lax.broadcasted_iota(jnp.int32, (tok_rows, tok_rows), 0)
    second_at = lax.broadcasted_iota(jnp.int32, (tok_rows, tok_rows), 1)
    earlier = (first < second_at).astype(jnp.float32).astype(jnp.bfloat16)
    before_row = jnp.dot(hits_row, earlier, preferred_element_type=jnp.float32)
    slot_row = [
        jnp.sum(jnp.where(ids_row[k : k + 1, :] == expert_col, before_row, 0.0), axis=0, keepdims=True)
        for k in range(2)
    ]
    slot_at = (
        lax.broadcasted_iota(jnp.int32, (slots, tok_rows), 0) - lead * core
    ).astype(jnp.float32)

    def pick_of(expert):
        taken = ((ids_row[0:1, :] == expert) & (slot_row[0] == slot_at)) | (
            (ids_row[1:2, :] == expert) & (slot_row[1] == slot_at)
        )
        return taken.astype(jnp.float32).astype(jnp.bfloat16)

    def picked(pick, where):
        return jnp.dot(pick, normed[:, where], preferred_element_type=jnp.float32).astype(
            jnp.bfloat16
        )

    with jax.named_scope("barrier"):
        pl.semaphore_wait(barrier, n_ep - 1 + 2)

    box_cols = {0: tp, 1: far, 2: tp, 3: tp, 4: side[0], 5: side[1]}

    def box_flip(box):
        return box if box in (2, 3) else 1

    def z_copy(box, c):
        return pltpu.make_async_remote_copy(
            src_ref=outbox.at[box, c],
            dst_ref=zbox.at[box, core],
            send_sem=z_send.at[box, c],
            recv_sem=z_recv.at[box, core],
            device_id=(flip(pair, box_flip(box)) * 2 + c, tp),
            device_id_type=pl.DeviceIdType.MESH,
        )

    def z_wait(box, cs=(0, 1)):
        for c in cs:
            pltpu.make_async_remote_copy(
                src_ref=outbox.at[0, c],
                dst_ref=zbox.at[box, c],
                send_sem=z_send.at[0, c],
                recv_sem=z_recv.at[box, c],
                device_id=(flip(pair, 1) * 2 + c, tp),
                device_id_type=pl.DeviceIdType.MESH,
            ).wait_recv()

    def z_sends(boxes_in_order):
        for box in boxes_in_order:
            where = pl.ds(pl.multiple_of(box_cols[box] * cols, cols), cols)
            for c in range(2):
                pick = pick_of(flip(pair, box_flip(box)) * 2 + c)
                outbox[box, c] = picked(pick, where)
                z_copy(box, c).start()

    with jax.named_scope("z_sends"):
        pl.when(inner == 1)(lambda: z_sends((2, 3, 0, 1)))
        pl.when(inner == 0)(lambda: z_sends((0, 1, 2, 3)))

    def norm_rest(i, carry):
        at = pl.ds(pl.multiple_of(i * 32, 32), 32)
        for other in side:
            where = pl.ds(pl.multiple_of(other * cols, cols), cols)
            values = tokens_ref[at, where].astype(jnp.float32)
            normed[at, where] = (values * scales[at, 0:1] * gain_ref[:, where]).astype(
                jnp.bfloat16
            )
        return carry

    with jax.named_scope("norm_rest"):
        lax.fori_loop(0, tok_rows // 32, norm_rest, 0)

    partner = flip(ep, 1)

    def pair_copy(at):
        return pltpu.make_async_remote_copy(
            src_ref=fullbox,
            dst_ref=zfull.at[at],
            send_sem=pair_send,
            recv_sem=pair_recv,
            device_id=(partner, tp),
            device_id_type=pl.DeviceIdType.MESH,
        )

    with jax.named_scope("pair_pick"):
        theirs = pick_of(partner)
        for j in range(n_tp):
            fullbox[j] = picked(theirs, slice(j * cols, (j + 1) * cols))
        pair_copy(core).start()
        mine = pick_of(ep)
        for j in range(n_tp):
            zfull[core, j] = picked(mine, slice(j * cols, (j + 1) * cols))

    z_sends((4, 5))
    edge = slots - second

    def join(k, j, low, high):
        xbuf[k, j, 0:second, :] = low[0:second, :]
        xbuf[k, j, second:slots, :] = low[second:slots, :] + high[0:edge, :]
        xbuf[k, j, slots:rows, :] = high[edge:slots, :]

    boxes = (xbuf, hbuf)
    half_cols = cols // 2
    spans = {0: (0, slots), 1: (slots, rows), None: (0, rows)}
    both = (0, 1)
    whole = (None,)
    far_parts = whole

    def g_copy(b, k, j, half, r, to, at):
        start, stop = spans[r]
        where = boxes[b].at[k, j, pl.ds(start, stop - start), pl.ds(half * half_cols, half_cols)]
        r = r or 0
        return pltpu.make_async_remote_copy(
            src_ref=where,
            dst_ref=where,
            send_sem=g_send.at[b, k, r, at],
            recv_sem=g_recv.at[b, k, r, at],
            device_id=(ep, to),
            device_id_type=pl.DeviceIdType.MESH,
        )

    def block_copy(b, k, d, half, r):
        return g_copy(b, k, tp, half, r, side[d], 2 * d + half)

    def block_arrival(b, k, d, half, r):
        return g_copy(b, k, side[d], half, r, side[d], 2 * d + half)

    def relay_copy(b, k, d, r):
        return g_copy(b, k, side[d], d, r, side[1 - d], 4 + d)

    def relay_arrival(b, k, d, r):
        return g_copy(b, k, far, d, r, side[1 - d], 4 + d)

    def spread_half(b, k, half, rs=whole):
        for r in rs:
            for d in range(2):
                block_copy(b, k, d, half, r).start()

    def spread(b, k, rs=whole):
        for r in rs:
            for step in range(2):
                for d in range(2):
                    block_copy(b, k, d, d if step == 0 else 1 - d, r).start()

    def relay(b, k, rs=whole, ds=both):
        for r in rs:
            for d in ds:
                with jax.named_scope(f"w_relay_{b}_{r}"):
                    block_arrival(b, k, d, d, r).wait_recv()
                relay_copy(b, k, d, r).start()

    def near(b, k, rs=whole):
        for r in rs:
            with jax.named_scope(f"w_near_{b}_{r}"):
                for d in range(2):
                    block_arrival(b, k, d, 1 - d, r).wait_recv()

    def distant(b, k, rs=whole):
        for r in rs:
            with jax.named_scope(f"w_far_{b}_{r}"):
                for d in range(2):
                    relay_arrival(b, k, d, r).wait_recv()

    def enter(k, rs=whole, wait=True):
        if wait:
            with jax.named_scope("w_z"):
                z_wait(k)
        join(k, tp, zbox[k, 0], zbox[k, 1])
        spread(0, k, rs)

    def enter_next():
        for box in (0, 1, 4, 5):
            with jax.named_scope("w_z1"):
                z_wait(box)
            join(1, box_cols[box], zbox[box, 0], zbox[box, 1])

    def dot_blocks(box, k, r, weight, where, blocks):
        depth = box.shape[-1]
        start, stop = spans[r]
        total = None
        for j in blocks:
            at = j * depth if isinstance(j, int) else pl.multiple_of(j * depth, depth)
            part = jnp.dot(
                box[k, j, start:stop, :], weight[pl.ds(at, depth), where],
                preferred_element_type=jnp.float32,
            )
            total = part if total is None else total + part
        return total

    every = tuple(range(n_tp))
    close = (tp,) + side

    def column(i):
        return pl.ds(pl.multiple_of(i * COLUMN_TILE, COLUMN_TILE), COLUMN_TILE)

    def units(k, part, r=None, parts=2, stage=None):
        start, stop = spans[r]
        blocks = {None: every, 0: close, 1: (far,)}[stage]

        def tile(i, carry):
            where = column(i)
            gate_pre = dot_blocks(xbuf, k, r, gate_v, where, blocks)
            up_pre = dot_blocks(xbuf, k, r, up_v, where, blocks)
            if stage == 0:
                acc[0, start:stop, where] = gate_pre
                acc[1, start:stop, where] = up_pre
                return carry
            if stage == 1:
                gate_pre = gate_pre + acc[0, start:stop, where]
                up_pre = up_pre + acc[1, start:stop, where]
            hbuf[k, tp, start:stop, where] = clamped_unit(gate_pre, up_pre)
            return carry

        tiles = hid // COLUMN_TILE // parts
        with jax.named_scope(f"units_{stage}_{r}"):
            lax.fori_loop(part * tiles, (part + 1) * tiles, tile, 0)

    def produce(k, r=None, stage=None):
        for half in range(2):
            units(k, half, r, 2, stage)
            spread_half(1, k, half, (r,))

    piece = outs // PIECES

    def piece_of(ref, at):
        return ref.at[:, pl.ds(at * piece, piece)]

    def back_copy(name, c, at):
        k = slot_of[name]
        return pltpu.make_async_remote_copy(
            src_ref=obuf.at[k, pl.ds(second * c, slots), pl.ds(at * piece, piece)],
            dst_ref=back.at[ep, :, pl.ds(at * piece, piece)],
            send_sem=b_send.at[k, c, at],
            recv_sem=b_recv.at[ep, at],
            device_id=(chip_of[name] * 2 + c, tp),
            device_id_type=pl.DeviceIdType.MESH,
        )

    def partner_copy(at):
        return pltpu.make_async_remote_copy(
            src_ref=obuf.at[
                0, pl.ds(pl.multiple_of(second * (1 - core), 8), slots), pl.ds(at * piece, piece)
            ],
            dst_ref=back.at[ep, :, pl.ds(at * piece, piece)],
            send_sem=b_send.at[0, 0, at],
            recv_sem=b_recv.at[ep, at],
            device_id=(partner, tp),
            device_id_type=pl.DeviceIdType.MESH,
        )

    def back_arrival(flips, at):
        other = flip(ep, flips)
        return pltpu.make_async_remote_copy(
            src_ref=obuf.at[0, pl.ds(0, slots), pl.ds(at * piece, piece)],
            dst_ref=back.at[other, :, pl.ds(at * piece, piece)],
            send_sem=b_send.at[0, 0, at],
            recv_sem=b_recv.at[other, at],
            device_id=(other, tp),
            device_id_type=pl.DeviceIdType.MESH,
        )

    def results(name, r=None, stage=None):
        k = slot_of[name]
        start, stop = spans[r]
        blocks = {None: every, 0: close, 1: (far,)}[stage]

        def tile(i, carry):
            where = column(i)
            total = dot_blocks(hbuf, k, r, down_v, where, blocks)
            if stage == 0:
                acc[2, start:stop, where] = total
                return carry
            if stage == 1:
                total = total + acc[2, start:stop, where]
            obuf[k, start:stop, where] = total.astype(jnp.bfloat16)
            return carry

        tiles = outs // COLUMN_TILE // PIECES
        for at in range(PIECES):
            with jax.named_scope(f"results_{name}_{stage}_{r}"):
                lax.fori_loop(at * tiles, (at + 1) * tiles, tile, 0)
            if stage == 0:
                continue
            if name == 0:
                partner_copy(at).start()
            else:
                for c in both if r is None else (r,):
                    back_copy(name, c, at).start()
        if name == 0 and stage != 0:
            back[ep] = obuf[0, pl.ds(pl.multiple_of(second * core, 8), slots), :]

    def begin(name, r=None):
        near(1, slot_of[name], (r,))
        results(name, r, 0)

    def finish(name, r=None):
        distant(1, slot_of[name], (r,))
        results(name, r, 1)

    with jax.named_scope("w_pair"):
        pair_copy(1 - core).wait_recv()
    for j in range(n_tp):
        join(0, j, zfull[0, j], zfull[1, j])
    with jax.named_scope("w_gateup"):
        loads[0].wait()
        loads[1].wait()
    units(0, 0)
    spread_half(1, 0, 0)
    units(0, 1)

    def outer_order():
        enter(2)
        relay(0, 2)
        near(0, 2)
        spread_half(1, 0, 1)
        units(2, 0, None, 1, 0)
        distant(0, 2)
        produce(2, None, 1)
        relay(1, 2)
        enter(3)
        loads[2].wait()
        begin("early")
        finish("early")
        relay(0, 3)
        relay(1, 0)
        near(0, 3)
        units(3, 0, None, 1, 0)
        distant(0, 3)
        produce(3, None, 1)
        enter_next()
        produce(1)
        relay(1, 3)
        begin("late")
        finish("late")
        relay(1, 1)
        begin(1)
        finish(1)
        begin(0)
        finish(0)

    def inner_order():
        enter(3)
        relay(0, 3)
        near(0, 3)
        spread_half(1, 0, 1)
        units(3, 0, None, 1, 0)
        distant(0, 3)
        produce(3, None, 1)
        relay(1, 3)
        enter(2)
        loads[2].wait()
        begin("early")
        finish("early")
        relay(0, 2)
        relay(1, 0)
        near(0, 2)
        units(2, 0, None, 1, 0)
        distant(0, 2)
        produce(2, None, 1)
        enter_next()
        produce(1)
        relay(1, 2)
        begin("late")
        finish("late")
        relay(1, 1)
        begin(1)
        finish(1)
        begin(0)
        finish(0)

    pl.when(inner == 0)(outer_order)
    pl.when(inner == 1)(inner_order)

    place = lax.broadcasted_iota(jnp.int32, (n_ep * slots, tok_rows), 0).astype(jnp.float32)
    share = None
    for k in range(2):
        spot = (
            ids_row[k : k + 1, :].astype(jnp.float32) * slots
            + slot_row[k]
            + (lead * core).astype(jnp.float32)
        )
        part = jnp.where(place == spot, route_row_ref[k : k + 1, :], 0.0)
        share = part if share is None else share + part
    share = jnp.transpose(share)
    share_high = share.astype(jnp.bfloat16)
    share_low = (share - share_high.astype(jnp.float32)).astype(jnp.bfloat16)

    with jax.named_scope("w_sends"):
        for box in range(6):
            for c in range(2):
                z_copy(box, c).wait_send()
        pair_copy(core).wait_send()
        for k in range(pairs):
            for b in range(2):
                if b == 0 and k < 2:
                    continue
                for d in range(2):
                    for r in far_parts if k > 1 else whole:
                        for half in range(2):
                            block_copy(b, k, d, half, r).wait_send()
                        relay_copy(b, k, d, r).wait_send()
        for at in range(PIECES):
            partner_copy(at).wait_send()
            for name in (1, "early", "late"):
                for c in range(2):
                    back_copy(name, c, at).wait_send()

    with jax.named_scope("w_back"):
        for at in range(PIECES):
            for flips in range(1, n_ep):
                back_arrival(flips, at).wait_recv()

    def mix(i, carry):
        where = pl.ds(pl.multiple_of(i * COLUMN_TILE, COLUMN_TILE), COLUMN_TILE)
        table = back[:, :, where].reshape(n_ep * slots, COLUMN_TILE)
        total = jnp.dot(share_high, table, preferred_element_type=jnp.float32)
        total = total + jnp.dot(share_low, table, preferred_element_type=jnp.float32)
        out_ref[:, where] = total.astype(jnp.bfloat16)
        return carry

    with jax.named_scope("mix"):
        lax.fori_loop(0, outs // COLUMN_TILE, mix, 0)


def fused_path(
    n_ep, n_tp, tokens, expert_ids, route_weight, norm_gain, gate_weight, up_weight, down_weight
):
    tok_rows, width = tokens.shape
    capacity, slots = slots_of(n_ep, tokens.shape, expert_ids.shape)
    rows = 2 * capacity
    hid = gate_weight.shape[2]
    outs = down_weight.shape[2]
    cols = width // n_tp
    pairs = n_ep // 2
    vmem = pl.BlockSpec(memory_space=pltpu.VMEM)
    hbm = pl.BlockSpec(memory_space=pltpu.HBM)
    dma = pltpu.SemaphoreType.DMA
    arrays = (
        tokens,
        jnp.transpose(expert_ids),
        jnp.transpose(route_weight),
        norm_gain.reshape(1, width),
        gate_weight,
        up_weight,
        down_weight,
    )
    return pl.pallas_call(
        functools.partial(fused_kernel, n_ep, n_tp, capacity, slots),
        out_shape=jax.ShapeDtypeStruct((tok_rows, outs), jnp.bfloat16),
        in_specs=[hbm] * 7,
        out_specs=vmem,
        scratch_shapes=[
            pltpu.VMEM(tokens.shape, tokens.dtype),
            pltpu.VMEM(expert_ids.shape[::-1], expert_ids.dtype),
            pltpu.VMEM(route_weight.shape[::-1], route_weight.dtype),
            pltpu.VMEM((1, width), norm_gain.dtype),
            pltpu.VMEM(gate_weight.shape[1:], jnp.bfloat16),
            pltpu.VMEM(up_weight.shape[1:], jnp.bfloat16),
            pltpu.VMEM(down_weight.shape[1:], jnp.bfloat16),
            pltpu.VMEM((tok_rows, 128), jnp.float32),
            pltpu.VMEM((tok_rows, width), jnp.bfloat16),
            pltpu.VMEM((pairs + 2, 2, slots, cols), jnp.bfloat16),
            pltpu.VMEM((n_tp, slots, cols), jnp.bfloat16),
            pltpu.VMEM((pairs + 2, 2, slots, cols), jnp.bfloat16),
            pltpu.VMEM((2, n_tp, slots, cols), jnp.bfloat16),
            pltpu.VMEM((pairs, n_tp, rows, cols), jnp.bfloat16),
            pltpu.VMEM((pairs, n_tp, rows, hid), jnp.bfloat16),
            pltpu.VMEM((pairs, rows, outs), jnp.bfloat16),
            pltpu.VMEM((n_ep, slots, outs), jnp.bfloat16),
            pltpu.VMEM((3, rows, hid), jnp.float32),
            dma((4,)),
            dma((3,)),
            dma((pairs + 2, 2)),
            dma((pairs + 2, 2)),
            dma,
            dma,
            dma((2, pairs, 2, 6)),
            dma((2, pairs, 2, 6)),
            dma((pairs, 2, PIECES)),
            dma((n_ep, PIECES)),
        ],
        compiler_params=pltpu.CompilerParams(
            collective_id=0, has_side_effects=True, vmem_limit_bytes=VMEM_BYTES
        ),
    )(*(pltpu.with_memory_space_constraint(array, pltpu.HBM) for array in arrays))


def slots_of(n_ep, token_shape, id_shape):
    capacity = 5 * token_shape[0] * id_shape[1] // (4 * n_ep)
    return capacity, -(-capacity // 8) * 8


def on_device(tokens, expert_ids, route_weight, norm_gain, gate_weight, up_weight, down_weight):
    n_ep = lax.axis_size("ep")
    n_tp = lax.axis_size("tp")
    args = (tokens, expert_ids, route_weight, norm_gain, gate_weight, up_weight, down_weight)
    fits = n_tp == 4 and n_ep == 8 and gate_weight.shape[0] == 1 and expert_ids.shape[1] == 2
    capacity, slots = slots_of(n_ep, tokens.shape, expert_ids.shape)
    if fits and capacity % 4 == 0 and slots > capacity:
        return fused_path(n_ep, n_tp, *args)
    return plain_path(*args)


def solution(mesh):
    placed = (
        P("ep", None),
        P("ep", None),
        P("ep", None),
        P(),
        P("ep", None, "tp"),
        P("ep", None, "tp"),
        P("ep", None, "tp"),
    )
    return jax.shard_map(
        on_device, mesh=mesh, in_specs=placed, out_specs=P("ep", "tp"), check_vma=False
    )
```

```python
import functools

import jax
import jax.numpy as jnp
from jax import lax
from jax.experimental import pallas as pl
from jax.experimental.pallas import tpu as pltpu
from jax.sharding import PartitionSpec as P

EPS = 1e-06
LIMIT = 7.0
ALPHA = 1.702


def rms_norm(tokens, norm_gain):
    values = tokens.astype(jnp.float32)
    scale = lax.rsqrt(jnp.mean(values * values, axis=-1, keepdims=True) + EPS)
    return (values * scale * norm_gain).astype(jnp.bfloat16)


def clamped_unit(gate_pre, up_pre):
    gate = jnp.minimum(gate_pre, LIMIT)
    up_part = jnp.clip(up_pre, -LIMIT, LIMIT)
    return ((up_part + 1.0) * gate * jax.nn.sigmoid(ALPHA * gate)).astype(jnp.bfloat16)


def slot_numbers(id_blocks, experts, capacity):
    onehot = (id_blocks[:, :, None] == jnp.arange(experts, dtype=jnp.int32)[None, None, :]).astype(
        jnp.int32
    )
    before = jnp.cumsum(onehot, axis=1) - onehot
    position = jnp.sum(before * onehot, axis=2)
    return id_blocks * capacity + position


def project_down(hidden, down_weight):
    result = jnp.einsum(
        "sejf,efd->sejd",
        lax.all_gather(hidden, "tp", axis=3, tiled=True),
        down_weight,
        preferred_element_type=jnp.float32,
    )
    return result.astype(jnp.bfloat16)


def plain_path(tokens, expert_ids, route_weight, norm_gain, gate_weight, up_weight, down_weight):
    n_ep = lax.axis_size("ep")
    n_tp = lax.axis_size("tp")
    tok_rows, width = tokens.shape
    top = expert_ids.shape[1]
    local_experts = gate_weight.shape[0]
    experts = local_experts * n_ep
    capacity = 5 * tok_rows * top // (4 * experts)
    cols = width // n_tp
    normed = rms_norm(tokens, norm_gain)
    dest = slot_numbers(expert_ids.reshape(1, tok_rows * top), experts, capacity).reshape(-1)
    slot_range = jnp.arange(experts * capacity, dtype=jnp.int32)
    match = slot_range[:, None] == dest[None, :]
    pick = jnp.any(match.reshape(experts * capacity, tok_rows, top), axis=2).astype(jnp.bfloat16)
    own = lax.dynamic_slice_in_dim(normed, lax.axis_index("tp") * cols, cols, 1)
    buffer = jnp.dot(pick, own, preferred_element_type=jnp.float32).astype(jnp.bfloat16)
    buffer = buffer.reshape(n_ep, local_experts, capacity, cols)
    arrived = lax.all_to_all(buffer, "ep", split_axis=0, concat_axis=0, tiled=True)
    piece = lax.all_gather(arrived, "tp", axis=3, tiled=True)
    gate_part = jnp.einsum("sejd,edf->sejf", piece, gate_weight, preferred_element_type=jnp.float32)
    up_part = jnp.einsum("sejd,edf->sejf", piece, up_weight, preferred_element_type=jnp.float32)
    hidden = clamped_unit(gate_part, up_part)
    result = project_down(hidden, down_weight)
    back = lax.all_to_all(result, "ep", split_axis=0, concat_axis=0, tiled=True).reshape(
        experts * capacity, cols
    )
    chosen = jnp.transpose(match).astype(jnp.bfloat16)
    per_copy = jnp.dot(chosen, back, preferred_element_type=jnp.float32).reshape(
        tok_rows, top, cols
    )
    mixed = jnp.sum(per_copy * route_weight[:, :, None], axis=1)
    return mixed.astype(jnp.bfloat16)


VMEM_BYTES = 47 * 1024 * 1024
COLUMN_TILE = 256
PIECES = 2


def flip(value, bits):
    bit = 1
    while bit <= bits:
        if bits & bit:
            value = value + bit - 2 * bit * lax.rem(lax.div(value, jnp.int32(bit)), jnp.int32(2))
        bit *= 2
    return value


def fused_kernel(
    n_ep,
    n_tp,
    capacity,
    slots,
    tokens_hbm,
    ids_row_hbm,
    route_row_hbm,
    gain_hbm,
    gate_hbm,
    up_hbm,
    down_hbm,
    out_ref,
    tokens_ref,
    ids_row_ref,
    route_row_ref,
    gain_ref,
    gate_v,
    up_v,
    down_v,
    scales,
    normed,
    outbox,
    fullbox,
    zbox,
    zfull,
    xbuf,
    hbuf,
    obuf,
    back,
    acc,
    mixed,
    small_sem,
    weight_sem,
    z_send,
    z_recv,
    pair_send,
    pair_recv,
    g_send,
    g_recv,
    b_send,
    b_recv,
):
    pairs = n_ep // 2
    rows = 2 * capacity
    lead = slots - capacity
    second = rows - slots
    tok_rows, width = tokens_ref.shape
    cols = xbuf.shape[-1]
    hid = hbuf.shape[-1]
    outs = obuf.shape[-1]
    ep = lax.axis_index("ep")
    tp = lax.axis_index("tp")
    pair = lax.div(ep, jnp.int32(2))
    core = lax.rem(ep, jnp.int32(2))
    side = (flip(tp, 1), flip(tp, 2))
    far = flip(tp, 3)
    inner = lax.rem(pair + lax.div(pair, jnp.int32(2)), jnp.int32(2))
    chip_of = [flip(pair, k) for k in range(pairs)]

    small = (
        (tokens_hbm, tokens_ref),
        (ids_row_hbm, ids_row_ref),
        (route_row_hbm, route_row_ref),
        (gain_hbm, gain_ref),
    )
    small_loads = [
        pltpu.make_async_copy(a, b, small_sem.at[i]) for i, (a, b) in enumerate(small)
    ]
    for load in small_loads:
        load.start()
    loads = [
        pltpu.make_async_copy(hbm.at[0], vmem, weight_sem.at[i])
        for i, (hbm, vmem) in enumerate(((gate_hbm, gate_v), (up_hbm, up_v), (down_hbm, down_v)))
    ]

    barrier = pltpu.get_barrier_semaphore()
    for k in range(1, n_ep):
        pl.semaphore_signal(
            barrier, inc=1, device_id=(flip(ep, k), tp), device_id_type=pl.DeviceIdType.MESH
        )
    for other in side:
        pl.semaphore_signal(
            barrier, inc=1, device_id=(ep, other), device_id_type=pl.DeviceIdType.MESH
        )

    with jax.named_scope("small_wait"):
        for load in small_loads:
            load.wait()
    for load in loads:
        load.start()

    own_cols = pl.ds(pl.multiple_of(tp * cols, cols), cols)
    far_cols = pl.ds(pl.multiple_of(far * cols, cols), cols)

    def scale_rows(i, carry):
        at = pl.ds(pl.multiple_of(i * 32, 32), 32)
        values = tokens_ref[at, :].astype(jnp.float32)
        scale = lax.rsqrt(jnp.mean(values * values, axis=-1, keepdims=True) + EPS)
        scales[at, :] = jnp.broadcast_to(scale, (32, scales.shape[1]))
        for where in (own_cols, far_cols):
            values = tokens_ref[at, where].astype(jnp.float32)
            normed[at, where] = (values * scale * gain_ref[:, where]).astype(jnp.bfloat16)
        return carry

    with jax.named_scope("scale_rows"):
        lax.fori_loop(0, tok_rows // 32, scale_rows, 0)

    ids_row = ids_row_ref[...]
    expert_col = lax.broadcasted_iota(jnp.int32, (n_ep, tok_rows), 0)
    hits_row = ((ids_row[0:1, :] == expert_col) | (ids_row[1:2, :] == expert_col)).astype(
        jnp.float32
    ).astype(jnp.bfloat16)
    first = lax.broadcasted_iota(jnp.int32, (tok_rows, tok_rows), 0)
    second_at = lax.broadcasted_iota(jnp.int32, (tok_rows, tok_rows), 1)
    earlier = (first < second_at).astype(jnp.float32).astype(jnp.bfloat16)
    before_row = jnp.dot(hits_row, earlier, preferred_element_type=jnp.float32)
    slot_row = [
        jnp.sum(jnp.where(ids_row[k : k + 1, :] == expert_col, before_row, 0.0), axis=0, keepdims=True)
        for k in range(2)
    ]
    slot_at = (
        lax.broadcasted_iota(jnp.int32, (slots, tok_rows), 0) - lead * core
    ).astype(jnp.float32)

    def pick_of(expert):
        taken = ((ids_row[0:1, :] == expert) & (slot_row[0] == slot_at)) | (
            (ids_row[1:2, :] == expert) & (slot_row[1] == slot_at)
        )
        return taken.astype(jnp.float32).astype(jnp.bfloat16)

    def picked(pick, where):
        return jnp.dot(pick, normed[:, where], preferred_element_type=jnp.float32).astype(
            jnp.bfloat16
        )

    with jax.named_scope("barrier"):
        pl.semaphore_wait(barrier, n_ep - 1 + 2)

    box_cols = (tp, tp, tp, far) + side + (far,)

    def box_flip(box):
        return {0: 2, 1: 3, 6: 3}.get(box, 1)

    def z_copy(box, c):
        return pltpu.make_async_remote_copy(
            src_ref=outbox.at[box, c],
            dst_ref=zbox.at[box, core],
            send_sem=z_send,
            recv_sem=z_recv.at[(0, 1, 2, 2, 3, 3, 4)[box]],
            device_id=(flip(pair, box_flip(box)) * 2 + c, tp),
            device_id_type=pl.DeviceIdType.MESH,
        )

    def bytes_of(ref, send, recv):
        return pltpu.make_async_remote_copy(
            src_ref=ref,
            dst_ref=ref,
            send_sem=send,
            recv_sem=recv,
            device_id=(ep, side[0]),
            device_id_type=pl.DeviceIdType.MESH,
        )

    def z_wait(at, ref):
        bytes_of(ref, z_send, z_recv.at[at]).wait_recv()

    def z_sends(boxes_in_order):
        for box in boxes_in_order:
            where = pl.ds(pl.multiple_of(box_cols[box] * cols, cols), cols)
            for c in range(2):
                pick = pick_of(flip(pair, box_flip(box)) * 2 + c)
                outbox[box, c] = picked(pick, where)
                z_copy(box, c).start()

    with jax.named_scope("z_sends"):
        pl.when(inner == 1)(lambda: z_sends((0, 1, 2)))
        pl.when(inner == 0)(lambda: z_sends((2, 0, 3, 1)))

    def norm_rest(i, carry):
        at = pl.ds(pl.multiple_of(i * 32, 32), 32)
        for other in side:
            where = pl.ds(pl.multiple_of(other * cols, cols), cols)
            values = tokens_ref[at, where].astype(jnp.float32)
            normed[at, where] = (values * scales[at, 0:1] * gain_ref[:, where]).astype(
                jnp.bfloat16
            )
        return carry

    with jax.named_scope("norm_rest"):
        lax.fori_loop(0, tok_rows // 32, norm_rest, 0)

    partner = flip(ep, 1)

    def pair_copy(at):
        return pltpu.make_async_remote_copy(
            src_ref=fullbox,
            dst_ref=zfull.at[at],
            send_sem=pair_send,
            recv_sem=pair_recv,
            device_id=(partner, tp),
            device_id_type=pl.DeviceIdType.MESH,
        )

    with jax.named_scope("pair_pick"):
        theirs = pick_of(partner)
        for j in range(n_tp):
            fullbox[j] = picked(theirs, slice(j * cols, (j + 1) * cols))
        pair_copy(core).start()
        mine = pick_of(ep)
        for j in range(n_tp):
            zfull[core, j] = picked(mine, slice(j * cols, (j + 1) * cols))

    edge = slots - second

    def join(k, j, low, high):
        xbuf[k, j, 0:second, :] = low[0:second, :]
        xbuf[k, j, second:slots, :] = low[second:slots, :] + high[0:edge, :]
        xbuf[k, j, slots:rows, :] = high[edge:slots, :]

    boxes = (xbuf, hbuf)
    half_cols = cols // 2
    spans = {0: (0, slots), 1: (slots, rows), None: (0, rows)}
    both = (0, 1)

    def group(b, k, r):
        return k - 2 if b == 0 else 2 + 2 * k + (r or 0)

    def g_copy(b, k, j, half, r, to, kind):
        start, stop = spans[r]
        where = boxes[b].at[k, j, pl.ds(start, stop - start), pl.ds(half * half_cols, half_cols)]
        return pltpu.make_async_remote_copy(
            src_ref=where,
            dst_ref=where,
            send_sem=g_send.at[b, k],
            recv_sem=g_recv.at[group(b, k, r), kind],
            device_id=(ep, to),
            device_id_type=pl.DeviceIdType.MESH,
        )

    def block_copy(b, k, d, half, r):
        return g_copy(b, k, tp, half, r, side[d], d if half == d and (b, k) != (0, 3) else 2)

    def take(b, k, r=None):
        for d in range(2):
            with jax.named_scope(f"w_relay_{b}_{r}"):
                g_copy(b, k, side[d], d, r, side[d], d).wait_recv()

    def hand(b, k, r=None):
        for d in range(2):
            g_copy(b, k, side[d], d, r, side[1 - d], 3).start()

    def relay(b, k, r=None):
        for d in range(2):
            with jax.named_scope(f"w_relay_{b}_{r}"):
                g_copy(b, k, side[d], d, r, side[d], d).wait_recv()
            g_copy(b, k, side[d], d, r, side[1 - d], 3).start()

    def arrive(b, k, r, kind):
        start, stop = spans[r]
        where = boxes[b].at[k, far, pl.ds(start, stop - start), :]
        bytes_of(where, g_send.at[b, k], g_recv.at[group(b, k, r), kind]).wait_recv()

    def send_half(b, k, half, r=None):
        for d in range(2):
            block_copy(b, k, d, half, r).start()

    def send_first(b, k, r=None):
        for d in range(2):
            block_copy(b, k, d, d, r).start()

    def send_rest(b, k, r=None):
        for d in range(2):
            block_copy(b, k, d, 1 - d, r).start()

    def spread(b, k, r=None):
        send_first(b, k, r)
        send_rest(b, k, r)

    def near(b, k, r=None):
        with jax.named_scope(f"w_near_{b}_{r}"):
            if (b, k) == (0, 3):
                bytes_of(xbuf.at[k, pl.ds(0, 2)], g_send.at[b, k], g_recv.at[1, 2]).wait_recv()
            else:
                arrive(b, k, r, 2)

    def distant(b, k, r=None):
        with jax.named_scope(f"w_far_{b}_{r}"):
            arrive(b, k, r, 3)

    def enter(k):
        with jax.named_scope("w_z"):
            z_wait(k - 2, zbox.at[k - 2])
        join(k, tp, zbox[k - 2, 0], zbox[k - 2, 1])

    def enter_far():
        with jax.named_scope("w_zfar"):
            z_wait(4, zbox.at[6])
        join(3, far, zbox[6, 0], zbox[6, 1])

    def enter_next(part):
        with jax.named_scope(f"w_z1_{part}"):
            z_wait(2 + part, zbox.at[pl.ds(2 + 2 * part, 2)])
        for box in range(2 + 2 * part, 4 + 2 * part):
            join(1, box_cols[box], zbox[box, 0], zbox[box, 1])

    def dot_blocks(box, k, r, weight, where, blocks):
        depth = box.shape[-1]
        start, stop = spans[r]
        total = None
        for j in blocks:
            at = j * depth if isinstance(j, int) else pl.multiple_of(j * depth, depth)
            part = jnp.dot(
                box[k, j, start:stop, :], weight[pl.ds(at, depth), where],
                preferred_element_type=jnp.float32,
            )
            total = part if total is None else total + part
        return total

    every = tuple(range(n_tp))
    close = (tp,) + side

    def column(i):
        return pl.ds(pl.multiple_of(i * COLUMN_TILE, COLUMN_TILE), COLUMN_TILE)

    stages = {
        None: (every, None, None),
        "near": (close, None, 0),
        "far": ((far,), 0, None),
        "own": ((tp, far), None, 2),
        "side": (side, 2, None),
        "own_last": ((tp, far), None, 0),
        "side_last": (side, 0, None),
    }

    def units(k, stage=None, halves=both):
        blocks, start, keep = stages[stage]

        def tile(i, carry):
            where = column(i)
            gate_pre = dot_blocks(xbuf, k, None, gate_v, where, blocks)
            up_pre = dot_blocks(xbuf, k, None, up_v, where, blocks)
            if start is not None:
                gate_pre = gate_pre + acc[start, :, where]
                up_pre = up_pre + acc[start + 1, :, where]
            if keep is not None:
                acc[keep, :, where] = gate_pre
                acc[keep + 1, :, where] = up_pre
            else:
                hbuf[k, tp, :, where] = clamped_unit(gate_pre, up_pre)
            return carry

        tiles = hid // COLUMN_TILE // 2
        with jax.named_scope(f"units_{stage}"):
            lax.fori_loop(halves[0] * tiles, (halves[-1] + 1) * tiles, tile, 0)

    def produce(k, stage, r=None):
        for half in both:
            units(k, stage, (half,))
            block_copy(1, k, half, half, r).start()
        send_rest(1, k, r)

    piece = outs // PIECES

    def piece_of(ref, at):
        return ref.at[:, pl.ds(at * piece, piece)]

    def back_send(k, start, to, at, group_at):
        return pltpu.make_async_remote_copy(
            src_ref=obuf.at[k, pl.ds(start, slots), pl.ds(at * piece, piece)],
            dst_ref=back.at[ep, :, pl.ds(at * piece, piece)],
            send_sem=b_send,
            recv_sem=b_recv.at[group_at],
            device_id=(to, tp),
            device_id_type=pl.DeviceIdType.MESH,
        )

    def results(name, stage, r=None):
        k = name
        start, stop = spans[r]
        blocks, _, keep = stages[stage]
        at_acc = 5 if name == 0 else 4

        def tile(i, carry):
            where = column(i)
            total = dot_blocks(hbuf, k, r, down_v, where, blocks)
            if keep is not None:
                acc[at_acc, start:stop, where] = total
                return carry
            total = total + acc[at_acc, start:stop, where]
            obuf[k, start:stop, where] = total.astype(jnp.bfloat16)
            return carry

        tiles = outs // COLUMN_TILE // PIECES
        for at in range(PIECES):
            with jax.named_scope(f"results_{name}_{stage}_{r}"):
                lax.fori_loop(at * tiles, (at + 1) * tiles, tile, 0)
            if keep is not None:
                continue
            if name == 0:
                back_send(0, pl.multiple_of(second * (1 - core), 8), partner, at, 0).start()
            else:
                for c in both if r is None else (r,):
                    back_send(k, second * c, chip_of[name] * 2 + c, at, int(name == 1)).start()
        if name == 0 and keep is None:
            back[ep] = obuf[0, pl.ds(pl.multiple_of(second * core, 8), slots), :]

    def begin(name, r=None):
        near(1, name, r)
        results(name, "near", r)

    def finish(name, r=None):
        distant(1, name, r)
        results(name, "far", r)

    mixed_chips = ((pair, chip_of[2], chip_of[3]), (chip_of[1],))

    def share_of(part):
        place = lax.broadcasted_iota(jnp.int32, (slots, tok_rows), 0)
        shares = []
        for chip in mixed_chips[part]:
            for c in both:
                share = None
                for k in range(2):
                    hit = (ids_row[k : k + 1, :] == chip * 2 + c) & (slot_row[k] == slot_at)
                    one = jnp.where(hit, route_row_ref[k : k + 1, :], 0.0)
                    share = one if share is None else share + one
                shares.append(share)
        share = jnp.transpose(jnp.concatenate(shares, axis=0))
        high = share.astype(jnp.bfloat16)
        low = (share - high.astype(jnp.float32)).astype(jnp.bfloat16)
        return jnp.concatenate([high, low], axis=1)

    def mix(part):
        share = share_of(part)
        with jax.named_scope(f"w_back_{part}"):
            got = back.at[pl.ds(0, 2 if part else 5)]
            bytes_of(got, b_send, b_recv.at[part]).wait_recv()

        def tile(i, carry):
            where = column(i)
            blocks = [back[chip * 2 + c, :, where] for chip in mixed_chips[part] for c in both]
            table = jnp.concatenate(blocks + blocks, axis=0)
            total = jnp.dot(share, table, preferred_element_type=jnp.float32)
            if part == 0:
                mixed[:, where] = total
            else:
                out_ref[:, where] = (mixed[:, where] + total).astype(jnp.bfloat16)
            return carry

        with jax.named_scope(f"mix_{part}"):
            lax.fori_loop(0, outs // COLUMN_TILE, tile, 0, unroll=True)

    def sends_done():
        with jax.named_scope("w_sends"):
            bytes_of(outbox, z_send, z_recv.at[0]).wait_send()
            pair_copy(core).wait_send()
            for b in range(2):
                for k in range(2 - 2 * b, pairs):
                    if (b, k) != (1, 1):
                        sent = boxes[b].at[k, pl.ds(0, 2 if (b, k) == (0, 3) else 3)]
                        bytes_of(sent, g_send.at[b, k], g_recv.at[0, 0]).wait_send()

    with jax.named_scope("w_pair"):
        pair_copy(1 - core).wait_recv()
    for j in range(n_tp):
        join(0, j, zfull[0, j], zfull[1, j])
    with jax.named_scope("w_gateup"):
        loads[0].wait()
        loads[1].wait()
    pl.when(inner == 1)(lambda: z_sends((3, 6)))
    units(0, None, (0,))
    send_half(1, 0, 0)
    units(0, None, (1,))

    def outer_order():
        z_sends((6, 4, 5))
        enter(2)
        spread(0, 2)
        relay(0, 2)
        near(0, 2)
        send_half(1, 0, 1)
        units(2, "near")
        distant(0, 2)
        produce(2, "far")
        enter_next(0)
        units(1, "own")
        loads[2].wait()
        take(1, 0)
        begin(0)
        relay(1, 2)
        enter(3)
        spread(0, 3)
        begin(2)
        finish(2)
        enter_far()
        units(3, "own_last")
        hand(1, 0)
        near(0, 3)
        produce(3, "side_last", 0)
        send_first(1, 3, 1)
        relay(1, 3, 0)
        send_rest(1, 3, 1)
        enter_next(1)
        units(1, "side")
        relay(1, 3, 1)
        spread(1, 1, 0)
        send_first(1, 1, 1)
        begin(3, 0)
        finish(3, 0)
        begin(3, 1)
        finish(3, 1)
        relay(1, 1, 0)
        send_rest(1, 1, 1)
        finish(0)
        begin(1, 0)
        relay(1, 1, 1)
        sends_done()
        finish(1, 0)
        begin(1, 1)
        finish(1, 1)
        mix(0)

    def inner_order():
        send_half(1, 0, 1)
        z_sends((4, 5))
        enter(2)
        spread(0, 2)
        relay(0, 2)
        near(0, 2)
        enter(3)
        send_first(0, 3)
        units(2, "near")
        distant(0, 2)
        produce(2, "far")
        enter_next(0)
        units(1, "own")
        loads[2].wait()
        take(1, 0)
        begin(0)
        relay(1, 2)
        send_rest(0, 3)
        begin(2)
        finish(2)
        enter_far()
        units(3, "own_last")
        hand(1, 0)
        near(0, 3)
        produce(3, "side_last", 0)
        send_first(1, 3, 1)
        relay(1, 3, 0)
        send_rest(1, 3, 1)
        enter_next(1)
        units(1, "side")
        relay(1, 3, 1)
        spread(1, 1, 0)
        send_first(1, 1, 1)
        begin(3, 0)
        finish(3, 0)
        begin(3, 1)
        finish(3, 1)
        relay(1, 1, 0)
        send_rest(1, 1, 1)
        finish(0)
        begin(1, 0)
        relay(1, 1, 1)
        sends_done()
        finish(1, 0)
        begin(1, 1)
        finish(1, 1)
        mix(0)

    pl.when(inner == 0)(outer_order)
    pl.when(inner == 1)(inner_order)

    with jax.named_scope("w_sends_2"):
        bytes_of(boxes[1].at[1, pl.ds(0, 3)], g_send.at[1, 1], g_recv.at[0, 0]).wait_send()
        bytes_of(back.at[pl.ds(0, n_ep - 1)], b_send, b_recv.at[0]).wait_send()
    mix(1)


def fused_path(
    n_ep, n_tp, tokens, expert_ids, route_weight, norm_gain, gate_weight, up_weight, down_weight
):
    tok_rows, width = tokens.shape
    capacity, slots = slots_of(n_ep, tokens.shape, expert_ids.shape)
    rows = 2 * capacity
    hid = gate_weight.shape[2]
    outs = down_weight.shape[2]
    cols = width // n_tp
    pairs = n_ep // 2
    vmem = pl.BlockSpec(memory_space=pltpu.VMEM)
    hbm = pl.BlockSpec(memory_space=pltpu.HBM)
    dma = pltpu.SemaphoreType.DMA
    arrays = (
        tokens,
        jnp.transpose(expert_ids),
        jnp.transpose(route_weight),
        norm_gain.reshape(1, width),
        gate_weight,
        up_weight,
        down_weight,
    )
    return pl.pallas_call(
        functools.partial(fused_kernel, n_ep, n_tp, capacity, slots),
        out_shape=jax.ShapeDtypeStruct((tok_rows, outs), jnp.bfloat16),
        in_specs=[hbm] * 7,
        out_specs=vmem,
        scratch_shapes=[
            pltpu.VMEM(tokens.shape, tokens.dtype),
            pltpu.VMEM(expert_ids.shape[::-1], expert_ids.dtype),
            pltpu.VMEM(route_weight.shape[::-1], route_weight.dtype),
            pltpu.VMEM((1, width), norm_gain.dtype),
            pltpu.VMEM(gate_weight.shape[1:], jnp.bfloat16),
            pltpu.VMEM(up_weight.shape[1:], jnp.bfloat16),
            pltpu.VMEM(down_weight.shape[1:], jnp.bfloat16),
            pltpu.VMEM((tok_rows, 128), jnp.float32),
            pltpu.VMEM((tok_rows, width), jnp.bfloat16),
            pltpu.VMEM((pairs + 3, 2, slots, cols), jnp.bfloat16),
            pltpu.VMEM((n_tp, slots, cols), jnp.bfloat16),
            pltpu.VMEM((pairs + 3, 2, slots, cols), jnp.bfloat16),
            pltpu.VMEM((2, n_tp, slots, cols), jnp.bfloat16),
            pltpu.VMEM((pairs, n_tp, rows, cols), jnp.bfloat16),
            pltpu.VMEM((pairs, n_tp, rows, hid), jnp.bfloat16),
            pltpu.VMEM((pairs, rows, outs), jnp.bfloat16),
            pltpu.VMEM((n_ep, slots, outs), jnp.bfloat16),
            pltpu.VMEM((6, rows, hid), jnp.float32),
            pltpu.VMEM((tok_rows, outs), jnp.float32),
            dma((4,)),
            dma((3,)),
            dma,
            dma((5,)),
            dma,
            dma,
            dma((2, pairs)),
            dma((2 + 2 * pairs, 4)),
            dma,
            dma((2,)),
        ],
        compiler_params=pltpu.CompilerParams(
            collective_id=0, has_side_effects=True, vmem_limit_bytes=VMEM_BYTES
        ),
    )(*(pltpu.with_memory_space_constraint(array, pltpu.HBM) for array in arrays))


def slots_of(n_ep, token_shape, id_shape):
    capacity = 5 * token_shape[0] * id_shape[1] // (4 * n_ep)
    return capacity, -(-capacity // 8) * 8


def on_device(tokens, expert_ids, route_weight, norm_gain, gate_weight, up_weight, down_weight):
    n_ep = lax.axis_size("ep")
    n_tp = lax.axis_size("tp")
    args = (tokens, expert_ids, route_weight, norm_gain, gate_weight, up_weight, down_weight)
    fits = n_tp == 4 and n_ep == 8 and gate_weight.shape[0] == 1 and expert_ids.shape[1] == 2
    capacity, slots = slots_of(n_ep, tokens.shape, expert_ids.shape)
    if fits and capacity % 4 == 0 and slots > capacity:
        return fused_path(n_ep, n_tp, *args)
    return plain_path(*args)


def solution(mesh):
    placed = (
        P("ep", None),
        P("ep", None),
        P("ep", None),
        P(),
        P("ep", None, "tp"),
        P("ep", None, "tp"),
        P("ep", None, "tp"),
    )
    return jax.shard_map(
        on_device, mesh=mesh, in_specs=placed, out_specs=P("ep", "tp"), check_vma=False
    )
```

```python
import functools

import jax
import jax.numpy as jnp
from jax import lax
from jax.experimental import pallas as pl
from jax.experimental.pallas import tpu as pltpu
from jax.sharding import PartitionSpec as P

EPS = 1e-06
LIMIT = 7.0
ALPHA = 1.702


def rms_norm(tokens, norm_gain):
    values = tokens.astype(jnp.float32)
    scale = lax.rsqrt(jnp.mean(values * values, axis=-1, keepdims=True) + EPS)
    return (values * scale * norm_gain).astype(jnp.bfloat16)


def clamped_unit(gate_pre, up_pre):
    gate = jnp.minimum(gate_pre, LIMIT)
    up_part = jnp.clip(up_pre, -LIMIT, LIMIT)
    return ((up_part + 1.0) * gate * jax.nn.sigmoid(ALPHA * gate)).astype(jnp.bfloat16)


def slot_numbers(id_blocks, experts, capacity):
    onehot = (id_blocks[:, :, None] == jnp.arange(experts, dtype=jnp.int32)[None, None, :]).astype(
        jnp.int32
    )
    before = jnp.cumsum(onehot, axis=1) - onehot
    position = jnp.sum(before * onehot, axis=2)
    return id_blocks * capacity + position


def project_down(hidden, down_weight):
    result = jnp.einsum(
        "sejf,efd->sejd",
        lax.all_gather(hidden, "tp", axis=3, tiled=True),
        down_weight,
        preferred_element_type=jnp.float32,
    )
    return result.astype(jnp.bfloat16)


def plain_path(tokens, expert_ids, route_weight, norm_gain, gate_weight, up_weight, down_weight):
    n_ep = lax.axis_size("ep")
    n_tp = lax.axis_size("tp")
    tok_rows, width = tokens.shape
    top = expert_ids.shape[1]
    local_experts = gate_weight.shape[0]
    experts = local_experts * n_ep
    capacity = 5 * tok_rows * top // (4 * experts)
    cols = width // n_tp
    normed = rms_norm(tokens, norm_gain)
    dest = slot_numbers(expert_ids.reshape(1, tok_rows * top), experts, capacity).reshape(-1)
    slot_range = jnp.arange(experts * capacity, dtype=jnp.int32)
    match = slot_range[:, None] == dest[None, :]
    pick = jnp.any(match.reshape(experts * capacity, tok_rows, top), axis=2).astype(jnp.bfloat16)
    own = lax.dynamic_slice_in_dim(normed, lax.axis_index("tp") * cols, cols, 1)
    buffer = jnp.dot(pick, own, preferred_element_type=jnp.float32).astype(jnp.bfloat16)
    buffer = buffer.reshape(n_ep, local_experts, capacity, cols)
    arrived = lax.all_to_all(buffer, "ep", split_axis=0, concat_axis=0, tiled=True)
    piece = lax.all_gather(arrived, "tp", axis=3, tiled=True)
    gate_part = jnp.einsum("sejd,edf->sejf", piece, gate_weight, preferred_element_type=jnp.float32)
    up_part = jnp.einsum("sejd,edf->sejf", piece, up_weight, preferred_element_type=jnp.float32)
    hidden = clamped_unit(gate_part, up_part)
    result = project_down(hidden, down_weight)
    back = lax.all_to_all(result, "ep", split_axis=0, concat_axis=0, tiled=True).reshape(
        experts * capacity, cols
    )
    chosen = jnp.transpose(match).astype(jnp.bfloat16)
    per_copy = jnp.dot(chosen, back, preferred_element_type=jnp.float32).reshape(
        tok_rows, top, cols
    )
    mixed = jnp.sum(per_copy * route_weight[:, :, None], axis=1)
    return mixed.astype(jnp.bfloat16)


VMEM_BYTES = 47 * 1024 * 1024
COLUMN_TILE = 256
PIECES = 2


def flip(value, bits):
    bit = 1
    while bit <= bits:
        if bits & bit:
            value = value + bit - 2 * bit * lax.rem(lax.div(value, jnp.int32(bit)), jnp.int32(2))
        bit *= 2
    return value


def fused_kernel(
    n_ep,
    n_tp,
    capacity,
    slots,
    tokens_hbm,
    ids_row_hbm,
    route_row_hbm,
    gain_hbm,
    gate_hbm,
    up_hbm,
    down_hbm,
    out_ref,
    tokens_ref,
    ids_row_ref,
    route_row_ref,
    gain_ref,
    gate_v,
    up_v,
    down_v,
    scales,
    normed,
    outbox,
    outedge,
    fullbox,
    fulledge,
    zedge,
    pairedge,
    xbuf,
    hbuf,
    obuf,
    obedge,
    back,
    backedge,
    acc,
    mixed,
    small_sem,
    weight_sem,
    z_send,
    z_recv,
    pair_send,
    pair_recv,
    g_send,
    g_recv,
    b_send,
    b_recv,
):
    pairs = n_ep // 2
    rows = 2 * capacity
    lead = slots - capacity
    second = rows - slots
    tok_rows, width = tokens_ref.shape
    cols = xbuf.shape[-1]
    hid = hbuf.shape[-1]
    outs = obuf.shape[-1]
    ep = lax.axis_index("ep")
    tp = lax.axis_index("tp")
    pair = lax.div(ep, jnp.int32(2))
    core = lax.rem(ep, jnp.int32(2))
    side = (flip(tp, 1), flip(tp, 2))
    far = flip(tp, 3)
    inner = lax.rem(pair + lax.div(pair, jnp.int32(2)), jnp.int32(2))
    chip_of = [flip(pair, k) for k in range(pairs)]

    top, low = pl.ds(0, tok_rows // 2), pl.ds(tok_rows // 2, tok_rows // 2)
    small = (
        (ids_row_hbm, ids_row_ref),
        (gain_hbm, gain_ref),
        (tokens_hbm.at[top], tokens_ref.at[top]),
        (tokens_hbm.at[low], tokens_ref.at[low]),
        (route_row_hbm, route_row_ref),
    )
    small_loads = [
        pltpu.make_async_copy(a, b, small_sem.at[i]) for i, (a, b) in enumerate(small)
    ]
    for load in small_loads:
        load.start()
    loads = [
        pltpu.make_async_copy(hbm.at[0], vmem, weight_sem.at[i])
        for i, (hbm, vmem) in enumerate(((gate_hbm, gate_v), (up_hbm, up_v), (down_hbm, down_v)))
    ]

    barrier = pltpu.get_barrier_semaphore()
    for k in range(1, n_ep):
        pl.semaphore_signal(
            barrier, inc=1, device_id=(flip(ep, k), tp), device_id_type=pl.DeviceIdType.MESH
        )
    for other in side:
        pl.semaphore_signal(
            barrier, inc=1, device_id=(ep, other), device_id_type=pl.DeviceIdType.MESH
        )

    own_cols = pl.ds(pl.multiple_of(tp * cols, cols), cols)
    far_cols = pl.ds(pl.multiple_of(far * cols, cols), cols)

    def scale_rows(i, carry):
        at = pl.ds(pl.multiple_of(i * 32, 32), 32)
        values = tokens_ref[at, :].astype(jnp.float32)
        scale = lax.rsqrt(jnp.mean(values * values, axis=-1, keepdims=True) + EPS)
        scales[at, :] = jnp.broadcast_to(scale, (32, scales.shape[1]))
        for where in (own_cols, far_cols):
            values = tokens_ref[at, where].astype(jnp.float32)
            normed[at, where] = (values * scale * gain_ref[:, where]).astype(jnp.bfloat16)
        return carry

    with jax.named_scope("small_wait"):
        small_loads[0].wait()

    ids_row = ids_row_ref[...]
    expert_col = lax.broadcasted_iota(jnp.int32, (n_ep, tok_rows), 0)
    hits_row = ((ids_row[0:1, :] == expert_col) | (ids_row[1:2, :] == expert_col)).astype(
        jnp.float32
    ).astype(jnp.bfloat16)
    first = lax.broadcasted_iota(jnp.int32, (tok_rows, tok_rows), 0)
    second_at = lax.broadcasted_iota(jnp.int32, (tok_rows, tok_rows), 1)
    earlier = (first < second_at).astype(jnp.float32).astype(jnp.bfloat16)
    before_row = jnp.dot(hits_row, earlier, preferred_element_type=jnp.float32)
    slot_row = [
        jnp.sum(jnp.where(ids_row[k : k + 1, :] == expert_col, before_row, 0.0), axis=0, keepdims=True)
        for k in range(2)
    ]
    block_row = lax.broadcasted_iota(jnp.int32, (slots, tok_rows), 0)
    edge_slot = second * (1 - core) - second

    def slots_at(shift):
        edge_row = block_row - shift
        at = jnp.where(
            block_row < second,
            block_row + lead * core,
            jnp.where((edge_row >= second) & (edge_row < capacity), edge_row + edge_slot, -1),
        )
        return at.astype(jnp.float32)

    slot_at = slots_at(0)

    def pick_of(expert):
        taken = ((ids_row[0:1, :] == expert) & (slot_row[0] == slot_at)) | (
            (ids_row[1:2, :] == expert) & (slot_row[1] == slot_at)
        )
        return taken.astype(jnp.float32).astype(jnp.bfloat16)

    def picked(pick, where):
        return jnp.dot(pick, normed[:, where], preferred_element_type=jnp.float32)

    with jax.named_scope("wait_top"):
        small_loads[1].wait()
        small_loads[2].wait()
    steps = tok_rows // 64
    with jax.named_scope("scale_top"):
        lax.fori_loop(0, steps, scale_rows, 0)
    with jax.named_scope("wait_low"):
        small_loads[3].wait()
        small_loads[4].wait()
    for load in loads:
        load.start()
    with jax.named_scope("scale_low"):
        lax.fori_loop(steps, 2 * steps, scale_rows, 0)

    box_cols = (tp, tp, tp, far) + side + (far,)

    def box_flip(box):
        return {0: 2, 1: 3, 6: 3}.get(box, 1)

    def mains(at):
        return pl.ds(pl.multiple_of(slots * at, 8), second)

    def z_copies(box, c):
        for src, dst in (
            (outbox.at[box, c], xbuf.at[box_flip(box), box_cols[box], mains(core)]),
            (outedge.at[box, c], zedge.at[box, core]),
        ):
            yield pltpu.make_async_remote_copy(
                src_ref=src,
                dst_ref=dst,
                send_sem=z_send.at[box // 4],
                recv_sem=z_recv.at[(0, 1, 2, 2, 3, 5, 4)[box]],
                device_id=(flip(pair, box_flip(box)) * 2 + c, tp),
                device_id_type=pl.DeviceIdType.MESH,
            )

    def bytes_of(ref, send, recv):
        return pltpu.make_async_remote_copy(
            src_ref=ref,
            dst_ref=ref,
            send_sem=send,
            recv_sem=recv,
            device_id=(ep, side[0]),
            device_id_type=pl.DeviceIdType.MESH,
        )

    def z_wait(at, ref):
        bytes_of(ref, z_send.at[0], z_recv.at[at]).wait_recv()

    def fold(values):
        return jnp.concatenate([values[:, : cols // 2], values[:, cols // 2 :]], axis=0)

    def z_fill(box):
        where = pl.ds(pl.multiple_of(box_cols[box] * cols, cols), cols)
        for c in range(2):
            values = picked(pick_of(flip(pair, box_flip(box)) * 2 + c), where)
            outbox[box, c] = values[:second].astype(jnp.bfloat16)
            outedge[box, c] = fold(values[second:capacity]).astype(jnp.bfloat16)

    def z_start(box):
        for c in range(2):
            for copy in z_copies(box, c):
                copy.start()

    def z_sends(boxes_in_order):
        for box in boxes_in_order:
            z_fill(box)
            z_start(box)

    def z_first(boxes_in_order):
        z_start(boxes_in_order[0])
        z_sends(boxes_in_order[1:])

    pl.when(inner == 1)(lambda: z_fill(0))
    pl.when(inner == 0)(lambda: z_fill(2))
    with jax.named_scope("barrier"):
        pl.semaphore_wait(barrier, n_ep - 1 + 2)


    with jax.named_scope("z_sends"):
        pl.when(inner == 1)(lambda: z_first((0, 1, 2)))
        pl.when(inner == 0)(lambda: z_first((2, 0, 3, 1)))

    def norm_rest(i, carry):
        at = pl.ds(pl.multiple_of(i * 32, 32), 32)
        for other in side:
            where = pl.ds(pl.multiple_of(other * cols, cols), cols)
            values = tokens_ref[at, where].astype(jnp.float32)
            normed[at, where] = (values * scales[at, 0:1] * gain_ref[:, where]).astype(
                jnp.bfloat16
            )
        return carry

    with jax.named_scope("norm_rest"):
        lax.fori_loop(0, tok_rows // 32, norm_rest, 0)

    partner = flip(ep, 1)

    def pair_copies():
        for src, dst in (
            (fullbox, xbuf.at[0, :, mains(core)]),
            (fulledge, pairedge.at[core]),
        ):
            yield pltpu.make_async_remote_copy(
                src_ref=src,
                dst_ref=dst,
                send_sem=pair_send,
                recv_sem=pair_recv,
                device_id=(partner, tp),
                device_id_type=pl.DeviceIdType.MESH,
            )

    with jax.named_scope("pair_pick"):
        theirs = pick_of(partner)
        for j in range(n_tp):
            values = picked(theirs, slice(j * cols, (j + 1) * cols))
            fullbox[j] = values[:second].astype(jnp.bfloat16)
            fulledge[j] = fold(values[second:capacity]).astype(jnp.bfloat16)
        for copy in pair_copies():
            copy.start()
        mine = pick_of(ep)
        for j in range(n_tp):
            values = picked(mine, slice(j * cols, (j + 1) * cols))
            xbuf[0, j, mains(core), :] = values[:second].astype(jnp.bfloat16)
            pairedge[core, j] = fold(values[second:capacity]).astype(jnp.bfloat16)

    def join(k, j, low, high):
        for half in range(2):
            mid = [v[lead * half : lead * half + lead, :] for v in (low, high)]
            lanes = slice(half * (cols // 2), (half + 1) * (cols // 2))
            xbuf[k, j, second:slots, lanes] = jnp.concatenate(mid, axis=0)

    boxes = (xbuf, hbuf)
    half_cols = cols // 2
    spans = {0: (0, slots), 1: (slots, rows), None: (0, rows)}
    both = (0, 1)

    def group(b, k, r):
        return k - 2 if b == 0 else 2 + 2 * k + (r or 0)

    def g_copy(b, k, j, half, r, to, kind):
        start, stop = spans[r]
        where = boxes[b].at[k, j, pl.ds(start, stop - start), pl.ds(half * half_cols, half_cols)]
        return pltpu.make_async_remote_copy(
            src_ref=where,
            dst_ref=where,
            send_sem=g_send.at[b, k],
            recv_sem=g_recv.at[group(b, k, r), kind],
            device_id=(ep, to),
            device_id_type=pl.DeviceIdType.MESH,
        )

    def block_copy(b, k, d, half, r):
        return g_copy(b, k, tp, half, r, side[d], d if half == d else 2)

    def take(b, k, r=None):
        for d in range(2):
            with jax.named_scope(f"w_relay_{b}_{r}"):
                g_copy(b, k, side[d], d, r, side[d], d).wait_recv()

    def hand(b, k, r=None):
        for d in range(2):
            g_copy(b, k, side[d], d, r, side[1 - d], 3).start()

    def relay(b, k, r=None):
        for d in range(2):
            with jax.named_scope(f"w_relay_{b}_{r}"):
                g_copy(b, k, side[d], d, r, side[d], d).wait_recv()
            g_copy(b, k, side[d], d, r, side[1 - d], 3).start()

    def arrive(b, k, r, kind):
        start, stop = spans[r]
        where = boxes[b].at[k, far, pl.ds(start, stop - start), :]
        bytes_of(where, g_send.at[b, k], g_recv.at[group(b, k, r), kind]).wait_recv()

    def send_half(b, k, half, r=None):
        for d in range(2):
            block_copy(b, k, d, half, r).start()

    def send_first(b, k, r=None):
        for d in range(2):
            block_copy(b, k, d, d, r).start()

    def send_rest(b, k, r=None):
        for d in range(2):
            block_copy(b, k, d, 1 - d, r).start()

    def spread(b, k, r=None):
        send_first(b, k, r)
        send_rest(b, k, r)

    def near(b, k, r=None):
        with jax.named_scope(f"w_near_{b}_{r}"):
            arrive(b, k, r, 2)

    def distant(b, k, r=None):
        with jax.named_scope(f"w_far_{b}_{r}"):
            arrive(b, k, r, 3)

    def enter(k):
        with jax.named_scope("w_z"):
            z_wait(k - 2, xbuf.at[k, tp])
        join(k, tp, zedge[k - 2, 0], zedge[k - 2, 1])

    def enter_far():
        with jax.named_scope("w_zfar"):
            z_wait(4, xbuf.at[3, far])
        join(3, far, zedge[6, 0], zedge[6, 1])

    def enter_next(part):
        first_box, count, at = ((2, 2, 2), (4, 1, 3), (5, 1, 5))[part]
        with jax.named_scope(f"w_z1_{part}"):
            z_wait(at, xbuf.at[1, pl.ds(0, count)])
        for box in range(first_box, first_box + count):
            join(1, box_cols[box], zedge[box, 0], zedge[box, 1])

    def dot_blocks(box, k, r, weight, where, blocks):
        depth = box.shape[-1]
        start, stop = spans[r]
        total = None
        for j, half in blocks:
            size = depth if half is None else depth // 2
            at = j * depth if isinstance(j, int) else pl.multiple_of(j * depth, depth)
            at = at + (half or 0) * size
            lanes = slice((half or 0) * size, (half or 0) * size + size)
            part = jnp.dot(
                box[k, j, start:stop, lanes], weight[pl.ds(at, size), where],
                preferred_element_type=jnp.float32,
            )
            total = part if total is None else total + part
        return total

    every = tuple((j, None) for j in range(n_tp))
    sides = tuple((j, None) for j in side)
    close = ((tp, None),) + sides

    def column(i):
        return pl.ds(pl.multiple_of(i * COLUMN_TILE, COLUMN_TILE), COLUMN_TILE)

    stages = {
        None: (every, None, None),
        "near": (close, None, 0),
        "far": (((far, None),), 0, None),
        "own": (((tp, None), (far, None)), None, 2),
        "third": (sides[:1], 2, 2),
        "fourth": (sides[1:], 2, None),
        "mine": (close[:1], None, 0),
        "sides": (sides, 0, 0),
        "own_last": (((tp, None), (far, None), (side[0], 0), (side[1], 1)), None, 0),
        "side_last": (((side[0], 1), (side[1], 0)), 0, None),
    }

    def units(k, stage=None, halves=both):
        blocks, start, keep = stages[stage]

        def tile(i, carry):
            where = column(i)
            gate_pre = dot_blocks(xbuf, k, None, gate_v, where, blocks)
            up_pre = dot_blocks(xbuf, k, None, up_v, where, blocks)
            if start is not None:
                gate_pre = gate_pre + acc[start, :, where]
                up_pre = up_pre + acc[start + 1, :, where]
            if keep is not None:
                acc[keep, :, where] = gate_pre
                acc[keep + 1, :, where] = up_pre
            else:
                hbuf[k, tp, :, where] = clamped_unit(gate_pre, up_pre)
            return carry

        tiles = hid // COLUMN_TILE // 2
        with jax.named_scope(f"units_{stage}"):
            lax.fori_loop(halves[0] * tiles, (halves[-1] + 1) * tiles, tile, 0)

    def produce(k, stage, r=None):
        for half in both:
            units(k, stage, (half,))
            block_copy(1, k, half, half, r).start()
        send_rest(1, k, r)

    piece = outs // PIECES

    def back_copy(src, dst, to, group_at):
        return pltpu.make_async_remote_copy(
            src_ref=src,
            dst_ref=dst,
            send_sem=b_send.at[group_at // 2],
            recv_sem=b_recv.at[group_at],
            device_id=(to, tp),
            device_id_type=pl.DeviceIdType.MESH,
        )

    def back_send(k, c, to, at, group_at):
        lanes = pl.ds(at * piece, piece)
        back_copy(obuf.at[k, mains(c), lanes], back.at[ep, :, lanes], to, group_at).start()
        if at == PIECES - 1:
            back_copy(obedge.at[k, c], backedge.at[ep], to, group_at).start()

    def results(name, stage, r=None):
        k = name
        start, stop = spans[r]
        blocks, begun, keep = stages[stage]
        at_acc = {0: 5, 1: 2}.get(name, 4)

        def tile(i, carry):
            where = column(i)
            total = dot_blocks(hbuf, k, r, down_v, where, blocks)
            if begun is not None:
                total = total + acc[at_acc, start:stop, where]
            if keep is not None:
                acc[at_acc, start:stop, where] = total
                return carry
            obuf[k, start:stop, where] = total.astype(jnp.bfloat16)
            return carry

        tiles = outs // COLUMN_TILE // PIECES
        for at in range(PIECES):
            with jax.named_scope(f"results_{name}_{stage}_{r}"):
                lax.fori_loop(at * tiles, (at + 1) * tiles, tile, 0)
            if keep is not None:
                continue
            if at == PIECES - 1 and r != 1:
                mid = obuf[k, second:slots, :].astype(jnp.float32)
                for c in both:
                    obedge[k, c] = fold(mid[lead * c : lead * c + lead]).astype(jnp.bfloat16)
            if name == 0:
                back_send(0, 1 - core, partner, at, 2)
            else:
                for c in both if r is None else (r,):
                    back_send(k, c, chip_of[name] * 2 + c, at, int(name == 1))
        if name == 0 and keep is None:
            back[ep] = obuf[0, mains(core), :]
            backedge[ep] = obedge[0, core]

    def begin(name, r=None):
        near(1, name, r)
        results(name, "near" if r is None else "sides", r)

    def finish(name, r=None):
        distant(1, name, r)
        results(name, "far", r)

    mixed_chips = ((pair, chip_of[2], chip_of[3]), (chip_of[1],))

    def share_of(part, at_slots):
        shares = []
        for chip in mixed_chips[part]:
            for c in both:
                share = None
                for k in range(2):
                    hit = (ids_row[k : k + 1, :] == chip * 2 + c) & (slot_row[k] == at_slots)
                    one = jnp.where(hit, route_row_ref[k : k + 1, :], 0.0)
                    share = one if share is None else share + one
                shares.append(share)
        share = jnp.transpose(jnp.concatenate(shares, axis=0))
        high = share.astype(jnp.bfloat16)
        low = (share - high.astype(jnp.float32)).astype(jnp.bfloat16)
        return jnp.concatenate([high, low], axis=1)

    def mix(part):
        shares = [share_of(part, at_slots) for at_slots in (slot_at, slots_at(lead))]
        with jax.named_scope(f"w_back_{part}"):
            if part == 0:
                half = obuf.at[0, :, pl.ds(0, outs // 2)]
                bytes_of(half, b_send.at[1], b_recv.at[2]).wait_recv()
            got = xbuf.at[0, pl.ds(0, 1 if part else 2)]
            bytes_of(got, b_send.at[0], b_recv.at[part]).wait_recv()
        with jax.named_scope(f"mix_{part}"):
            for i in range(outs // COLUMN_TILE):
                where = slice(i * COLUMN_TILE, (i + 1) * COLUMN_TILE)
                half = i * COLUMN_TILE // (outs // 2)
                lanes = slice(where.start - half * (outs // 2), where.stop - half * (outs // 2))
                blocks = []
                for chip in mixed_chips[part]:
                    for c in both:
                        blocks += [back[chip * 2 + c, :, where], backedge[chip * 2 + c, :, lanes]]
                table = jnp.concatenate(blocks + blocks, axis=0)
                total = jnp.dot(shares[half], table, preferred_element_type=jnp.float32)
                if part == 0:
                    mixed[:, where] = total
                else:
                    out_ref[:, where] = (mixed[:, where] + total).astype(jnp.bfloat16)

    def sends_done():
        with jax.named_scope("w_sends"):
            bytes_of(xbuf.at[0], z_send.at[0], z_recv.at[0]).wait_send()
            bytes_of(xbuf.at[0, pl.ds(0, 3)], z_send.at[1], z_recv.at[0]).wait_send()
            bytes_of(xbuf.at[0, pl.ds(0, 2)], pair_send, z_recv.at[0]).wait_send()
            half = obuf.at[0, :, pl.ds(0, outs // 2)]
            bytes_of(half, b_send.at[1], b_recv.at[2]).wait_send()
            for b in range(2):
                for k in range(2 - 2 * b, pairs):
                    if (b, k) != (1, 1):
                        sent = boxes[b].at[k, pl.ds(0, 2 if (b, k) == (0, 3) else 3)]
                        bytes_of(sent, g_send.at[b, k], g_recv.at[0, 0]).wait_send()

    with jax.named_scope("w_pair"):
        bytes_of(xbuf.at[0, pl.ds(0, 2)], pair_send, pair_recv).wait_recv()
    for j in range(n_tp):
        join(0, j, pairedge[0, j], pairedge[1, j])
    with jax.named_scope("w_gateup"):
        loads[0].wait()
        loads[1].wait()
    pl.when(inner == 1)(lambda: z_sends((3, 6)))
    units(0, None, (0,))
    send_half(1, 0, 0)
    units(0, None, (1,))

    def outer_order():
        z_sends((6, 4, 5))
        enter(2)
        spread(0, 2)
        relay(0, 2)
        near(0, 2)
        send_half(1, 0, 1)
        units(2, "near")
        distant(0, 2)
        produce(2, "far")
        enter_next(0)
        units(1, "own")
        loads[2].wait()
        take(1, 0)
        begin(0)
        relay(1, 2)
        enter(3)
        spread(0, 3)
        begin(2)
        finish(2)
        hand(1, 0)
        enter_far()
        take(0, 3)
        units(3, "own_last")
        near(0, 3)
        produce(3, "side_last", 0)
        send_first(1, 3, 1)
        finish(0)
        results(3, "mine")
        relay(1, 3, 0)
        send_rest(1, 3, 1)
        enter_next(1)
        units(1, "third")
        relay(1, 3, 1)
        enter_next(2)
        produce(1, "fourth", 0)
        send_first(1, 1, 1)
        begin(3, 0)
        finish(3, 0)
        begin(3, 1)
        relay(1, 1, 0)
        send_rest(1, 1, 1)
        finish(3, 1)
        results(1, "mine")
        relay(1, 1, 1)
        begin(1, 0)
        sends_done()
        finish(1, 0)
        begin(1, 1)
        finish(1, 1)
        mix(0)

    def inner_order():
        send_half(1, 0, 1)
        z_sends((4, 5))
        enter(2)
        spread(0, 2)
        relay(0, 2)
        near(0, 2)
        enter(3)
        send_first(0, 3)
        units(2, "near")
        distant(0, 2)
        produce(2, "far")
        enter_next(0)
        units(1, "own")
        loads[2].wait()
        take(1, 0)
        begin(0)
        relay(1, 2)
        send_rest(0, 3)
        begin(2)
        finish(2)
        hand(1, 0)
        enter_far()
        take(0, 3)
        units(3, "own_last")
        near(0, 3)
        produce(3, "side_last", 0)
        send_first(1, 3, 1)
        finish(0)
        results(3, "mine")
        relay(1, 3, 0)
        send_rest(1, 3, 1)
        enter_next(1)
        units(1, "third")
        relay(1, 3, 1)
        enter_next(2)
        produce(1, "fourth", 0)
        send_first(1, 1, 1)
        begin(3, 0)
        finish(3, 0)
        begin(3, 1)
        relay(1, 1, 0)
        send_rest(1, 1, 1)
        finish(3, 1)
        results(1, "mine")
        relay(1, 1, 1)
        begin(1, 0)
        sends_done()
        finish(1, 0)
        begin(1, 1)
        finish(1, 1)
        mix(0)

    pl.when(inner == 0)(outer_order)
    pl.when(inner == 1)(inner_order)

    with jax.named_scope("w_sends_2"):
        bytes_of(boxes[1].at[1, pl.ds(0, 3)], g_send.at[1, 1], g_recv.at[0, 0]).wait_send()
        bytes_of(xbuf.at[0, pl.ds(0, 3)], b_send.at[0], b_recv.at[0]).wait_send()
    mix(1)


def fused_path(
    n_ep, n_tp, tokens, expert_ids, route_weight, norm_gain, gate_weight, up_weight, down_weight
):
    tok_rows, width = tokens.shape
    capacity, slots = slots_of(n_ep, tokens.shape, expert_ids.shape)
    rows = 2 * capacity
    main, edge = rows - slots, 2 * (slots - capacity)
    hid = gate_weight.shape[2]
    outs = down_weight.shape[2]
    cols = width // n_tp
    pairs = n_ep // 2
    vmem = pl.BlockSpec(memory_space=pltpu.VMEM)
    hbm = pl.BlockSpec(memory_space=pltpu.HBM)
    dma = pltpu.SemaphoreType.DMA
    arrays = (
        tokens,
        jnp.transpose(expert_ids),
        jnp.transpose(route_weight),
        norm_gain.reshape(1, width),
        gate_weight,
        up_weight,
        down_weight,
    )
    return pl.pallas_call(
        functools.partial(fused_kernel, n_ep, n_tp, capacity, slots),
        out_shape=jax.ShapeDtypeStruct((tok_rows, outs), jnp.bfloat16),
        in_specs=[hbm] * 7,
        out_specs=vmem,
        scratch_shapes=[
            pltpu.VMEM(tokens.shape, tokens.dtype),
            pltpu.VMEM(expert_ids.shape[::-1], expert_ids.dtype),
            pltpu.VMEM(route_weight.shape[::-1], route_weight.dtype),
            pltpu.VMEM((1, width), norm_gain.dtype),
            pltpu.VMEM(gate_weight.shape[1:], jnp.bfloat16),
            pltpu.VMEM(up_weight.shape[1:], jnp.bfloat16),
            pltpu.VMEM(down_weight.shape[1:], jnp.bfloat16),
            pltpu.VMEM((tok_rows, 128), jnp.float32),
            pltpu.VMEM((tok_rows, width), jnp.bfloat16),
            pltpu.VMEM((pairs + 3, 2, main, cols), jnp.bfloat16),
            pltpu.VMEM((pairs + 3, 2, edge, cols // 2), jnp.bfloat16),
            pltpu.VMEM((n_tp, main, cols), jnp.bfloat16),
            pltpu.VMEM((n_tp, edge, cols // 2), jnp.bfloat16),
            pltpu.VMEM((pairs + 3, 2, edge, cols // 2), jnp.bfloat16),
            pltpu.VMEM((2, n_tp, edge, cols // 2), jnp.bfloat16),
            pltpu.VMEM((pairs, n_tp, rows, cols), jnp.bfloat16),
            pltpu.VMEM((pairs, n_tp, rows, hid), jnp.bfloat16),
            pltpu.VMEM((pairs, rows, outs), jnp.bfloat16),
            pltpu.VMEM((pairs, 2, edge, outs // 2), jnp.bfloat16),
            pltpu.VMEM((n_ep, main, outs), jnp.bfloat16),
            pltpu.VMEM((n_ep, edge, outs // 2), jnp.bfloat16),
            pltpu.VMEM((6, rows, hid), jnp.float32),
            pltpu.VMEM((tok_rows, outs), jnp.float32),
            dma((5,)),
            dma((3,)),
            dma((2,)),
            dma((6,)),
            dma,
            dma,
            dma((2, pairs)),
            dma((2 + 2 * pairs, 4)),
            dma((2,)),
            dma((3,)),
        ],
        compiler_params=pltpu.CompilerParams(
            collective_id=0, has_side_effects=True, vmem_limit_bytes=VMEM_BYTES
        ),
    )(*(pltpu.with_memory_space_constraint(array, pltpu.HBM) for array in arrays))


def slots_of(n_ep, token_shape, id_shape):
    capacity = 5 * token_shape[0] * id_shape[1] // (4 * n_ep)
    return capacity, -(-capacity // 8) * 8


def on_device(tokens, expert_ids, route_weight, norm_gain, gate_weight, up_weight, down_weight):
    n_ep = lax.axis_size("ep")
    n_tp = lax.axis_size("tp")
    args = (tokens, expert_ids, route_weight, norm_gain, gate_weight, up_weight, down_weight)
    fits = n_tp == 4 and n_ep == 8 and gate_weight.shape[0] == 1 and expert_ids.shape[1] == 2
    capacity, slots = slots_of(n_ep, tokens.shape, expert_ids.shape)
    cols = tokens.shape[1] // n_tp
    even = gate_weight.shape[2] == cols and down_weight.shape[2] == cols
    if fits and even and capacity % 4 == 0 and slots - capacity == 4:
        return fused_path(n_ep, n_tp, *args)
    return plain_path(*args)


def solution(mesh):
    placed = (
        P("ep", None),
        P("ep", None),
        P("ep", None),
        P(),
        P("ep", None, "tp"),
        P("ep", None, "tp"),
        P("ep", None, "tp"),
    )
    return jax.shard_map(
        on_device, mesh=mesh, in_specs=placed, out_specs=P("ep", "tp"), check_vma=False
    )
```

```python
import functools

import jax
import jax.numpy as jnp
from jax import lax
from jax.experimental import pallas as pl
from jax.experimental.pallas import tpu as pltpu
from jax.sharding import PartitionSpec as P

EPS = 1e-06
LIMIT = 7.0
ALPHA = 1.702


def rms_norm(tokens, norm_gain):
    values = tokens.astype(jnp.float32)
    scale = lax.rsqrt(jnp.mean(values * values, axis=-1, keepdims=True) + EPS)
    return (values * scale * norm_gain).astype(jnp.bfloat16)


def clamped_unit(gate_pre, up_pre):
    gate = jnp.minimum(gate_pre, LIMIT)
    up_part = jnp.clip(up_pre, -LIMIT, LIMIT)
    return ((up_part + 1.0) * gate * jax.nn.sigmoid(ALPHA * gate)).astype(jnp.bfloat16)


def slot_numbers(id_blocks, experts, capacity):
    onehot = (id_blocks[:, :, None] == jnp.arange(experts, dtype=jnp.int32)[None, None, :]).astype(
        jnp.int32
    )
    before = jnp.cumsum(onehot, axis=1) - onehot
    position = jnp.sum(before * onehot, axis=2)
    return id_blocks * capacity + position


def project_down(hidden, down_weight):
    result = jnp.einsum(
        "sejf,efd->sejd",
        lax.all_gather(hidden, "tp", axis=3, tiled=True),
        down_weight,
        preferred_element_type=jnp.float32,
    )
    return result.astype(jnp.bfloat16)


def plain_path(tokens, expert_ids, route_weight, norm_gain, gate_weight, up_weight, down_weight):
    n_ep = lax.axis_size("ep")
    n_tp = lax.axis_size("tp")
    tok_rows, width = tokens.shape
    top = expert_ids.shape[1]
    local_experts = gate_weight.shape[0]
    experts = local_experts * n_ep
    capacity = 5 * tok_rows * top // (4 * experts)
    cols = width // n_tp
    normed = rms_norm(tokens, norm_gain)
    dest = slot_numbers(expert_ids.reshape(1, tok_rows * top), experts, capacity).reshape(-1)
    slot_range = jnp.arange(experts * capacity, dtype=jnp.int32)
    match = slot_range[:, None] == dest[None, :]
    pick = jnp.any(match.reshape(experts * capacity, tok_rows, top), axis=2).astype(jnp.bfloat16)
    own = lax.dynamic_slice_in_dim(normed, lax.axis_index("tp") * cols, cols, 1)
    buffer = jnp.dot(pick, own, preferred_element_type=jnp.float32).astype(jnp.bfloat16)
    buffer = buffer.reshape(n_ep, local_experts, capacity, cols)
    arrived = lax.all_to_all(buffer, "ep", split_axis=0, concat_axis=0, tiled=True)
    piece = lax.all_gather(arrived, "tp", axis=3, tiled=True)
    gate_part = jnp.einsum("sejd,edf->sejf", piece, gate_weight, preferred_element_type=jnp.float32)
    up_part = jnp.einsum("sejd,edf->sejf", piece, up_weight, preferred_element_type=jnp.float32)
    hidden = clamped_unit(gate_part, up_part)
    result = project_down(hidden, down_weight)
    back = lax.all_to_all(result, "ep", split_axis=0, concat_axis=0, tiled=True).reshape(
        experts * capacity, cols
    )
    chosen = jnp.transpose(match).astype(jnp.bfloat16)
    per_copy = jnp.dot(chosen, back, preferred_element_type=jnp.float32).reshape(
        tok_rows, top, cols
    )
    mixed = jnp.sum(per_copy * route_weight[:, :, None], axis=1)
    return mixed.astype(jnp.bfloat16)


VMEM_BYTES = 47 * 1024 * 1024
COLUMN_TILE = 256
PIECES = 2


def flip(value, bits):
    bit = 1
    while bit <= bits:
        if bits & bit:
            value = value + bit - 2 * bit * lax.rem(lax.div(value, jnp.int32(bit)), jnp.int32(2))
        bit *= 2
    return value


def fused_kernel(
    n_ep,
    n_tp,
    capacity,
    slots,
    tokens_hbm,
    ids_row_hbm,
    route_row_hbm,
    gain_hbm,
    gate_hbm,
    up_hbm,
    down_hbm,
    out_ref,
    tokens_ref,
    ids_row_ref,
    route_row_ref,
    gain_ref,
    gate_v,
    up_v,
    down_v,
    scales,
    normed,
    outbox,
    outedge,
    fullbox,
    fulledge,
    zedge,
    pairedge,
    xbuf,
    hbuf,
    obuf,
    obedge,
    back,
    backedge,
    acc,
    mixed,
    small_sem,
    weight_sem,
    z_send,
    z_recv,
    pair_send,
    pair_recv,
    g_send,
    g_recv,
    b_send,
    b_recv,
):
    pairs = n_ep // 2
    rows = 2 * capacity
    lead = slots - capacity
    second = rows - slots
    tok_rows, width = tokens_ref.shape
    cols = xbuf.shape[-1]
    hid = hbuf.shape[-1]
    outs = obuf.shape[-1]
    ep = lax.axis_index("ep")
    tp = lax.axis_index("tp")
    pair = lax.div(ep, jnp.int32(2))
    core = lax.rem(ep, jnp.int32(2))
    side = (flip(tp, 1), flip(tp, 2))
    far = flip(tp, 3)
    inner = lax.rem(pair + lax.div(pair, jnp.int32(2)), jnp.int32(2))
    chip_of = [flip(pair, k) for k in range(pairs)]

    top, low = pl.ds(0, tok_rows // 2), pl.ds(tok_rows // 2, tok_rows // 2)
    small = (
        (ids_row_hbm, ids_row_ref),
        (gain_hbm, gain_ref),
        (tokens_hbm.at[top], tokens_ref.at[top]),
        (tokens_hbm.at[low], tokens_ref.at[low]),
        (route_row_hbm, route_row_ref),
    )
    small_loads = [
        pltpu.make_async_copy(a, b, small_sem.at[i]) for i, (a, b) in enumerate(small)
    ]
    for load in small_loads:
        load.start()
    half_hid = hid // 2
    parts = [
        (hbm.at[0, :, lanes], vmem.at[:, lanes])
        for lanes in (pl.ds(0, half_hid), pl.ds(half_hid, half_hid))
        for hbm, vmem in ((gate_hbm, gate_v), (up_hbm, up_v))
    ]
    parts.append((down_hbm.at[0], down_v))
    loads = [pltpu.make_async_copy(a, b, weight_sem.at[i]) for i, (a, b) in enumerate(parts)]

    barrier = pltpu.get_barrier_semaphore()
    for k in range(1, n_ep):
        pl.semaphore_signal(
            barrier, inc=1, device_id=(flip(ep, k), tp), device_id_type=pl.DeviceIdType.MESH
        )
    for other in side:
        pl.semaphore_signal(
            barrier, inc=1, device_id=(ep, other), device_id_type=pl.DeviceIdType.MESH
        )

    own_cols = pl.ds(pl.multiple_of(tp * cols, cols), cols)
    far_cols = pl.ds(pl.multiple_of(far * cols, cols), cols)

    def scale_rows(i, carry):
        at = pl.ds(pl.multiple_of(i * 32, 32), 32)
        values = tokens_ref[at, :].astype(jnp.float32)
        scale = lax.rsqrt(jnp.mean(values * values, axis=-1, keepdims=True) + EPS)
        scales[at, :] = jnp.broadcast_to(scale, (32, scales.shape[1]))
        for where in (own_cols, far_cols):
            values = tokens_ref[at, where].astype(jnp.float32)
            normed[at, where] = (values * scale * gain_ref[:, where]).astype(jnp.bfloat16)
        return carry

    with jax.named_scope("small_wait"):
        small_loads[0].wait()

    ids_row = ids_row_ref[...]
    expert_col = lax.broadcasted_iota(jnp.int32, (n_ep, tok_rows), 0)
    hits_row = ((ids_row[0:1, :] == expert_col) | (ids_row[1:2, :] == expert_col)).astype(
        jnp.float32
    ).astype(jnp.bfloat16)
    first = lax.broadcasted_iota(jnp.int32, (tok_rows, tok_rows), 0)
    second_at = lax.broadcasted_iota(jnp.int32, (tok_rows, tok_rows), 1)
    earlier = (first < second_at).astype(jnp.float32).astype(jnp.bfloat16)
    before_row = jnp.dot(hits_row, earlier, preferred_element_type=jnp.float32)
    slot_row = [
        jnp.sum(jnp.where(ids_row[k : k + 1, :] == expert_col, before_row, 0.0), axis=0, keepdims=True)
        for k in range(2)
    ]
    block_row = lax.broadcasted_iota(jnp.int32, (slots, tok_rows), 0)
    edge_slot = second * (1 - core) - second

    def slots_at(shift):
        edge_row = block_row - shift
        at = jnp.where(
            block_row < second,
            block_row + lead * core,
            jnp.where((edge_row >= second) & (edge_row < capacity), edge_row + edge_slot, -1),
        )
        return at.astype(jnp.float32)

    slot_at = slots_at(0)

    def pick_of(expert):
        taken = ((ids_row[0:1, :] == expert) & (slot_row[0] == slot_at)) | (
            (ids_row[1:2, :] == expert) & (slot_row[1] == slot_at)
        )
        return taken.astype(jnp.float32).astype(jnp.bfloat16)

    def picked(pick, where):
        return jnp.dot(pick, normed[:, where], preferred_element_type=jnp.float32)

    with jax.named_scope("wait_top"):
        small_loads[1].wait()
        small_loads[2].wait()
    steps = tok_rows // 64
    with jax.named_scope("scale_top"):
        lax.fori_loop(0, steps, scale_rows, 0)
    with jax.named_scope("wait_low"):
        small_loads[3].wait()
        small_loads[4].wait()
    for load in loads:
        load.start()
    with jax.named_scope("scale_low"):
        lax.fori_loop(steps, 2 * steps, scale_rows, 0)

    box_cols = (tp, tp, tp, far) + side + (far,)

    def box_flip(box):
        return {0: 2, 1: 3, 6: 3}.get(box, 1)

    def mains(at):
        return pl.ds(pl.multiple_of(slots * at, 8), second)

    def z_copies(box, c):
        for src, dst in (
            (outbox.at[box, c], xbuf.at[box_flip(box), box_cols[box], mains(core)]),
            (outedge.at[box, c], zedge.at[box, core]),
        ):
            yield pltpu.make_async_remote_copy(
                src_ref=src,
                dst_ref=dst,
                send_sem=z_send.at[box // 4],
                recv_sem=z_recv.at[(0, 1, 2, 2, 3, 5, 4)[box]],
                device_id=(flip(pair, box_flip(box)) * 2 + c, tp),
                device_id_type=pl.DeviceIdType.MESH,
            )

    def bytes_of(ref, send, recv):
        return pltpu.make_async_remote_copy(
            src_ref=ref,
            dst_ref=ref,
            send_sem=send,
            recv_sem=recv,
            device_id=(ep, side[0]),
            device_id_type=pl.DeviceIdType.MESH,
        )

    def z_wait(at, ref):
        bytes_of(ref, z_send.at[0], z_recv.at[at]).wait_recv()

    def fold(values):
        return jnp.concatenate([values[:, : cols // 2], values[:, cols // 2 :]], axis=0)

    def z_fill(box):
        where = pl.ds(pl.multiple_of(box_cols[box] * cols, cols), cols)
        for c in range(2):
            values = picked(pick_of(flip(pair, box_flip(box)) * 2 + c), where)
            outbox[box, c] = values[:second].astype(jnp.bfloat16)
            outedge[box, c] = fold(values[second:capacity]).astype(jnp.bfloat16)

    def z_start(box, cs=(0, 1)):
        for c in cs:
            for copy in z_copies(box, c):
                copy.start()

    def z_sends(boxes_in_order):
        for box in boxes_in_order:
            z_fill(box)
            z_start(box)

    def norm_rest(i, carry):
        at = pl.ds(pl.multiple_of(i * 32, 32), 32)
        for other in side:
            where = pl.ds(pl.multiple_of(other * cols, cols), cols)
            values = tokens_ref[at, where].astype(jnp.float32)
            normed[at, where] = (values * scales[at, 0:1] * gain_ref[:, where]).astype(
                jnp.bfloat16
            )
        return carry

    partner = flip(ep, 1)

    def pair_copies():
        for src, dst in (
            (fullbox, xbuf.at[0, :, mains(core)]),
            (fulledge, pairedge.at[core]),
        ):
            yield pltpu.make_async_remote_copy(
                src_ref=src,
                dst_ref=dst,
                send_sem=pair_send,
                recv_sem=pair_recv,
                device_id=(partner, tp),
                device_id_type=pl.DeviceIdType.MESH,
            )

    def pair_fill():
        lax.fori_loop(0, tok_rows // 32, norm_rest, 0)
        theirs = pick_of(partner)
        for j in range(n_tp):
            values = picked(theirs, slice(j * cols, (j + 1) * cols))
            fullbox[j] = values[:second].astype(jnp.bfloat16)
            fulledge[j] = fold(values[second:capacity]).astype(jnp.bfloat16)

    def outer_fill():
        z_fill(2)
        z_fill(0)

    def outer_sends():
        for c in range(2):
            z_start(2, (c,))
            z_start(0, (c,))
        pair_fill()

    def inner_sends():
        z_start(0)
        z_sends((2,))
        pair_fill()

    with jax.named_scope("fill"):
        pl.when(inner == 1)(lambda: z_fill(0))
        pl.when(inner == 0)(outer_fill)
    with jax.named_scope("barrier"):
        pl.semaphore_wait(barrier, n_ep - 1 + 2)
    with jax.named_scope("z_sends"):
        pl.when(inner == 1)(inner_sends)
        pl.when(inner == 0)(outer_sends)
    with jax.named_scope("pair_pick"):
        for copy in pair_copies():
            copy.start()
        mine = pick_of(ep)
        for j in range(n_tp):
            values = picked(mine, slice(j * cols, (j + 1) * cols))
            xbuf[0, j, mains(core), :] = values[:second].astype(jnp.bfloat16)
            pairedge[core, j] = fold(values[second:capacity]).astype(jnp.bfloat16)
        pl.when(inner == 1)(lambda: z_sends((1,)))
        pl.when(inner == 0)(lambda: z_sends((3, 1)))

    def join(k, j, low, high):
        for half in range(2):
            mid = [v[lead * half : lead * half + lead, :] for v in (low, high)]
            lanes = slice(half * (cols // 2), (half + 1) * (cols // 2))
            xbuf[k, j, second:slots, lanes] = jnp.concatenate(mid, axis=0)

    boxes = (xbuf, hbuf)
    half_cols = cols // 2
    spans = {0: (0, slots), 1: (slots, rows), None: (0, rows)}
    both = (0, 1)

    def group(b, k, r):
        return k - 2 if b == 0 else 2 + 2 * k + (r or 0)

    def g_copy(b, k, j, half, r, to, kind):
        start, stop = spans[r]
        where = boxes[b].at[k, j, pl.ds(start, stop - start), pl.ds(half * half_cols, half_cols)]
        return pltpu.make_async_remote_copy(
            src_ref=where,
            dst_ref=where,
            send_sem=g_send.at[b, k],
            recv_sem=g_recv.at[group(b, k, r), kind],
            device_id=(ep, to),
            device_id_type=pl.DeviceIdType.MESH,
        )

    def block_copy(b, k, d, half, r):
        return g_copy(b, k, tp, half, r, side[d], d if half == d else 2)

    def take(b, k, r=None):
        for d in range(2):
            with jax.named_scope(f"w_relay_{b}_{r}"):
                g_copy(b, k, side[d], d, r, side[d], d).wait_recv()

    def hand(b, k, r=None):
        for d in range(2):
            g_copy(b, k, side[d], d, r, side[1 - d], 3).start()

    def relay(b, k, r=None):
        for d in range(2):
            with jax.named_scope(f"w_relay_{b}_{r}"):
                g_copy(b, k, side[d], d, r, side[d], d).wait_recv()
            g_copy(b, k, side[d], d, r, side[1 - d], 3).start()

    def arrive(b, k, r, kind):
        start, stop = spans[r]
        where = boxes[b].at[k, far, pl.ds(start, stop - start), :]
        bytes_of(where, g_send.at[b, k], g_recv.at[group(b, k, r), kind]).wait_recv()

    def send_half(b, k, half, r=None):
        for d in range(2):
            block_copy(b, k, d, half, r).start()

    def send_first(b, k, r=None):
        for d in range(2):
            block_copy(b, k, d, d, r).start()

    def send_rest(b, k, r=None):
        for d in range(2):
            block_copy(b, k, d, 1 - d, r).start()

    def spread(b, k, r=None):
        send_first(b, k, r)
        send_rest(b, k, r)

    def near(b, k, r=None):
        with jax.named_scope(f"w_near_{b}_{r}"):
            arrive(b, k, r, 2)

    def distant(b, k, r=None):
        with jax.named_scope(f"w_far_{b}_{r}"):
            arrive(b, k, r, 3)

    def enter(k):
        with jax.named_scope("w_z"):
            z_wait(k - 2, xbuf.at[k, tp])
        join(k, tp, zedge[k - 2, 0], zedge[k - 2, 1])

    def enter_far():
        with jax.named_scope("w_zfar"):
            z_wait(4, xbuf.at[3, far])
        join(3, far, zedge[6, 0], zedge[6, 1])

    def enter_next(part):
        first_box, count, at = ((2, 2, 2), (4, 1, 3), (5, 1, 5))[part]
        with jax.named_scope(f"w_z1_{part}"):
            z_wait(at, xbuf.at[1, pl.ds(0, count)])
        for box in range(first_box, first_box + count):
            join(1, box_cols[box], zedge[box, 0], zedge[box, 1])

    def dot_blocks(box, k, r, weight, where, blocks):
        depth = box.shape[-1]
        start, stop = spans[r]
        total = None
        for j, half in blocks:
            size = depth if half is None else depth // 2
            at = j * depth if isinstance(j, int) else pl.multiple_of(j * depth, depth)
            at = at + (half or 0) * size
            lanes = slice((half or 0) * size, (half or 0) * size + size)
            part = jnp.dot(
                box[k, j, start:stop, lanes], weight[pl.ds(at, size), where],
                preferred_element_type=jnp.float32,
            )
            total = part if total is None else total + part
        return total

    every = tuple((j, None) for j in range(n_tp))
    sides = tuple((j, None) for j in side)
    close = ((tp, None),) + sides

    def column(i):
        return pl.ds(pl.multiple_of(i * COLUMN_TILE, COLUMN_TILE), COLUMN_TILE)

    stages = {
        None: (every, None, None),
        "near": (close, None, 0),
        "far": (((far, None),), 0, None),
        "own": (((tp, None), (far, None)), None, 2),
        "third": (sides[:1], 2, 2),
        "fourth": (sides[1:], 2, None),
        "mine": (close[:1], None, 0),
        "sides": (sides, 0, 0),
        "own_last": (((tp, None), (far, None), (side[0], 0), (side[1], 1)), None, 0),
        "side_last": (((side[0], 1), (side[1], 0)), 0, None),
    }

    def units(k, stage=None, halves=both):
        blocks, start, keep = stages[stage]

        def tile(i, carry):
            where = column(i)
            gate_pre = dot_blocks(xbuf, k, None, gate_v, where, blocks)
            up_pre = dot_blocks(xbuf, k, None, up_v, where, blocks)
            if start is not None:
                gate_pre = gate_pre + acc[start, :, where]
                up_pre = up_pre + acc[start + 1, :, where]
            if keep is not None:
                acc[keep, :, where] = gate_pre
                acc[keep + 1, :, where] = up_pre
            else:
                hbuf[k, tp, :, where] = clamped_unit(gate_pre, up_pre)
            return carry

        tiles = hid // COLUMN_TILE // 2
        with jax.named_scope(f"units_{stage}"):
            lax.fori_loop(halves[0] * tiles, (halves[-1] + 1) * tiles, tile, 0)

    def produce(k, stage, r=None):
        for half in both:
            units(k, stage, (half,))
            block_copy(1, k, half, half, r).start()
        send_rest(1, k, r)

    piece = outs // PIECES

    def back_copy(src, dst, to, group_at):
        return pltpu.make_async_remote_copy(
            src_ref=src,
            dst_ref=dst,
            send_sem=b_send.at[group_at // 2],
            recv_sem=b_recv.at[group_at],
            device_id=(to, tp),
            device_id_type=pl.DeviceIdType.MESH,
        )

    def back_send(k, c, to, at, group_at):
        lanes = pl.ds(at * piece, piece)
        back_copy(obuf.at[k, mains(c), lanes], back.at[ep, :, lanes], to, group_at).start()
        if at == PIECES - 1:
            back_copy(obedge.at[k, c], backedge.at[ep], to, group_at).start()

    def results(name, stage, r=None):
        k = name
        start, stop = spans[r]
        blocks, begun, keep = stages[stage]
        at_acc = {0: 5, 1: 2}.get(name, 4)

        def tile(i, carry):
            where = column(i)
            total = dot_blocks(hbuf, k, r, down_v, where, blocks)
            if begun is not None:
                total = total + acc[at_acc, start:stop, where]
            if keep is not None:
                acc[at_acc, start:stop, where] = total
                return carry
            obuf[k, start:stop, where] = total.astype(jnp.bfloat16)
            return carry

        tiles = outs // COLUMN_TILE // PIECES
        for at in range(PIECES):
            with jax.named_scope(f"results_{name}_{stage}_{r}"):
                lax.fori_loop(at * tiles, (at + 1) * tiles, tile, 0)
            if keep is not None:
                continue
            if at == PIECES - 1 and r != 1:
                mid = obuf[k, second:slots, :].astype(jnp.float32)
                for c in both:
                    obedge[k, c] = fold(mid[lead * c : lead * c + lead]).astype(jnp.bfloat16)
            if name == 0:
                back_send(0, 1 - core, partner, at, 2)
            else:
                for c in both if r is None else (r,):
                    back_send(k, c, chip_of[name] * 2 + c, at, int(name == 1))
        if name == 0 and keep is None:
            back[ep] = obuf[0, mains(core), :]
            backedge[ep] = obedge[0, core]

    def begin(name, r=None):
        near(1, name, r)
        results(name, "near" if r is None else "sides", r)

    def finish(name, r=None):
        distant(1, name, r)
        results(name, "far", r)

    mixed_chips = ((pair, chip_of[2], chip_of[3]), (chip_of[1],))

    def share_of(part, at_slots):
        shares = []
        for chip in mixed_chips[part]:
            for c in both:
                share = None
                for k in range(2):
                    hit = (ids_row[k : k + 1, :] == chip * 2 + c) & (slot_row[k] == at_slots)
                    one = jnp.where(hit, route_row_ref[k : k + 1, :], 0.0)
                    share = one if share is None else share + one
                shares.append(share)
        share = jnp.transpose(jnp.concatenate(shares, axis=0))
        high = share.astype(jnp.bfloat16)
        low = (share - high.astype(jnp.float32)).astype(jnp.bfloat16)
        return jnp.concatenate([high, low], axis=1)

    def mix(part):
        shares = [share_of(part, at_slots) for at_slots in (slot_at, slots_at(lead))]
        with jax.named_scope(f"w_back_{part}"):
            if part == 0:
                half = obuf.at[0, :, pl.ds(0, outs // 2)]
                bytes_of(half, b_send.at[1], b_recv.at[2]).wait_recv()
            got = xbuf.at[0, pl.ds(0, 1 if part else 2)]
            bytes_of(got, b_send.at[0], b_recv.at[part]).wait_recv()
        with jax.named_scope(f"mix_{part}"):
            for i in range(outs // COLUMN_TILE):
                where = slice(i * COLUMN_TILE, (i + 1) * COLUMN_TILE)
                half = i * COLUMN_TILE // (outs // 2)
                lanes = slice(where.start - half * (outs // 2), where.stop - half * (outs // 2))
                blocks = []
                for chip in mixed_chips[part]:
                    for c in both:
                        blocks += [back[chip * 2 + c, :, where], backedge[chip * 2 + c, :, lanes]]
                table = jnp.concatenate(blocks + blocks, axis=0)
                total = jnp.dot(shares[half], table, preferred_element_type=jnp.float32)
                if part == 0:
                    mixed[:, where] = total
                else:
                    out_ref[:, where] = (mixed[:, where] + total).astype(jnp.bfloat16)

    def sends_done():
        with jax.named_scope("w_sends"):
            bytes_of(xbuf.at[0], z_send.at[0], z_recv.at[0]).wait_send()
            bytes_of(xbuf.at[0, pl.ds(0, 3)], z_send.at[1], z_recv.at[0]).wait_send()
            bytes_of(xbuf.at[0, pl.ds(0, 2)], pair_send, z_recv.at[0]).wait_send()
            half = obuf.at[0, :, pl.ds(0, outs // 2)]
            bytes_of(half, b_send.at[1], b_recv.at[2]).wait_send()
            for b in range(2):
                for k in range(2 - 2 * b, pairs):
                    if (b, k) != (1, 1):
                        sent = boxes[b].at[k, pl.ds(0, 2 if (b, k) == (0, 3) else 3)]
                        bytes_of(sent, g_send.at[b, k], g_recv.at[0, 0]).wait_send()

    with jax.named_scope("w_pair"):
        bytes_of(xbuf.at[0, pl.ds(0, 2)], pair_send, pair_recv).wait_recv()
    for j in range(n_tp):
        join(0, j, pairedge[0, j], pairedge[1, j])
    with jax.named_scope("w_gateup"):
        loads[0].wait()
        loads[1].wait()
    units(0, None, (0,))
    send_half(1, 0, 0)
    pl.when(inner == 1)(lambda: z_sends((3, 6)))
    with jax.named_scope("w_gateup"):
        loads[2].wait()
        loads[3].wait()
    units(0, None, (1,))

    def outer_order():
        z_sends((6, 4, 5))
        enter(2)
        spread(0, 2)
        relay(0, 2)
        near(0, 2)
        send_half(1, 0, 1)
        units(2, "near")
        distant(0, 2)
        produce(2, "far")
        enter_next(0)
        units(1, "own")
        loads[4].wait()
        take(1, 0)
        begin(0)
        relay(1, 2)
        enter(3)
        spread(0, 3)
        begin(2)
        finish(2)
        hand(1, 0)
        enter_far()
        take(0, 3)
        units(3, "own_last")
        near(0, 3)
        produce(3, "side_last", 0)
        send_first(1, 3, 1)
        finish(0)
        results(3, "mine")
        relay(1, 3, 0)
        send_rest(1, 3, 1)
        enter_next(1)
        units(1, "third")
        relay(1, 3, 1)
        enter_next(2)
        produce(1, "fourth", 0)
        send_first(1, 1, 1)
        begin(3, 0)
        finish(3, 0)
        begin(3, 1)
        relay(1, 1, 0)
        send_rest(1, 1, 1)
        finish(3, 1)
        results(1, "mine")
        relay(1, 1, 1)
        begin(1, 0)
        sends_done()
        finish(1, 0)
        begin(1, 1)
        finish(1, 1)
        mix(0)

    def inner_order():
        send_half(1, 0, 1)
        z_sends((4, 5))
        enter(2)
        spread(0, 2)
        relay(0, 2)
        near(0, 2)
        enter(3)
        send_first(0, 3)
        units(2, "near")
        distant(0, 2)
        produce(2, "far")
        enter_next(0)
        units(1, "own")
        loads[4].wait()
        take(1, 0)
        begin(0)
        relay(1, 2)
        send_rest(0, 3)
        begin(2)
        finish(2)
        hand(1, 0)
        enter_far()
        take(0, 3)
        units(3, "own_last")
        near(0, 3)
        produce(3, "side_last", 0)
        send_first(1, 3, 1)
        finish(0)
        results(3, "mine")
        relay(1, 3, 0)
        send_rest(1, 3, 1)
        enter_next(1)
        units(1, "third")
        relay(1, 3, 1)
        enter_next(2)
        produce(1, "fourth", 0)
        send_first(1, 1, 1)
        begin(3, 0)
        finish(3, 0)
        begin(3, 1)
        relay(1, 1, 0)
        send_rest(1, 1, 1)
        finish(3, 1)
        results(1, "mine")
        relay(1, 1, 1)
        begin(1, 0)
        sends_done()
        finish(1, 0)
        begin(1, 1)
        finish(1, 1)
        mix(0)

    pl.when(inner == 0)(outer_order)
    pl.when(inner == 1)(inner_order)

    with jax.named_scope("w_sends_2"):
        bytes_of(boxes[1].at[1, pl.ds(0, 3)], g_send.at[1, 1], g_recv.at[0, 0]).wait_send()
        bytes_of(xbuf.at[0, pl.ds(0, 3)], b_send.at[0], b_recv.at[0]).wait_send()
    mix(1)


def fused_path(
    n_ep, n_tp, tokens, expert_ids, route_weight, norm_gain, gate_weight, up_weight, down_weight
):
    tok_rows, width = tokens.shape
    capacity, slots = slots_of(n_ep, tokens.shape, expert_ids.shape)
    rows = 2 * capacity
    main, edge = rows - slots, 2 * (slots - capacity)
    hid = gate_weight.shape[2]
    outs = down_weight.shape[2]
    cols = width // n_tp
    pairs = n_ep // 2
    vmem = pl.BlockSpec(memory_space=pltpu.VMEM)
    hbm = pl.BlockSpec(memory_space=pltpu.HBM)
    dma = pltpu.SemaphoreType.DMA
    arrays = (
        tokens,
        jnp.transpose(expert_ids),
        jnp.transpose(route_weight),
        norm_gain.reshape(1, width),
        gate_weight,
        up_weight,
        down_weight,
    )
    return pl.pallas_call(
        functools.partial(fused_kernel, n_ep, n_tp, capacity, slots),
        out_shape=jax.ShapeDtypeStruct((tok_rows, outs), jnp.bfloat16),
        in_specs=[hbm] * 7,
        out_specs=vmem,
        scratch_shapes=[
            pltpu.VMEM(tokens.shape, tokens.dtype),
            pltpu.VMEM(expert_ids.shape[::-1], expert_ids.dtype),
            pltpu.VMEM(route_weight.shape[::-1], route_weight.dtype),
            pltpu.VMEM((1, width), norm_gain.dtype),
            pltpu.VMEM(gate_weight.shape[1:], jnp.bfloat16),
            pltpu.VMEM(up_weight.shape[1:], jnp.bfloat16),
            pltpu.VMEM(down_weight.shape[1:], jnp.bfloat16),
            pltpu.VMEM((tok_rows, 128), jnp.float32),
            pltpu.VMEM((tok_rows, width), jnp.bfloat16),
            pltpu.VMEM((pairs + 3, 2, main, cols), jnp.bfloat16),
            pltpu.VMEM((pairs + 3, 2, edge, cols // 2), jnp.bfloat16),
            pltpu.VMEM((n_tp, main, cols), jnp.bfloat16),
            pltpu.VMEM((n_tp, edge, cols // 2), jnp.bfloat16),
            pltpu.VMEM((pairs + 3, 2, edge, cols // 2), jnp.bfloat16),
            pltpu.VMEM((2, n_tp, edge, cols // 2), jnp.bfloat16),
            pltpu.VMEM((pairs, n_tp, rows, cols), jnp.bfloat16),
            pltpu.VMEM((pairs, n_tp, rows, hid), jnp.bfloat16),
            pltpu.VMEM((pairs, rows, outs), jnp.bfloat16),
            pltpu.VMEM((pairs, 2, edge, outs // 2), jnp.bfloat16),
            pltpu.VMEM((n_ep, main, outs), jnp.bfloat16),
            pltpu.VMEM((n_ep, edge, outs // 2), jnp.bfloat16),
            pltpu.VMEM((6, rows, hid), jnp.float32),
            pltpu.VMEM((tok_rows, outs), jnp.float32),
            dma((5,)),
            dma((5,)),
            dma((2,)),
            dma((6,)),
            dma,
            dma,
            dma((2, pairs)),
            dma((2 + 2 * pairs, 4)),
            dma((2,)),
            dma((3,)),
        ],
        compiler_params=pltpu.CompilerParams(
            collective_id=0, has_side_effects=True, vmem_limit_bytes=VMEM_BYTES
        ),
    )(*(pltpu.with_memory_space_constraint(array, pltpu.HBM) for array in arrays))


def slots_of(n_ep, token_shape, id_shape):
    capacity = 5 * token_shape[0] * id_shape[1] // (4 * n_ep)
    return capacity, -(-capacity // 8) * 8


def on_device(tokens, expert_ids, route_weight, norm_gain, gate_weight, up_weight, down_weight):
    n_ep = lax.axis_size("ep")
    n_tp = lax.axis_size("tp")
    args = (tokens, expert_ids, route_weight, norm_gain, gate_weight, up_weight, down_weight)
    fits = n_tp == 4 and n_ep == 8 and gate_weight.shape[0] == 1 and expert_ids.shape[1] == 2
    capacity, slots = slots_of(n_ep, tokens.shape, expert_ids.shape)
    cols = tokens.shape[1] // n_tp
    even = gate_weight.shape[2] == cols and down_weight.shape[2] == cols
    if fits and even and capacity % 4 == 0 and slots - capacity == 4:
        return fused_path(n_ep, n_tp, *args)
    return plain_path(*args)


def solution(mesh):
    placed = (
        P("ep", None),
        P("ep", None),
        P("ep", None),
        P(),
        P("ep", None, "tp"),
        P("ep", None, "tp"),
        P("ep", None, "tp"),
    )
    return jax.shard_map(
        on_device, mesh=mesh, in_specs=placed, out_specs=P("ep", "tp"), check_vma=False
    )
```

```python
import functools

import jax
import jax.numpy as jnp
from jax import lax
from jax.experimental import pallas as pl
from jax.experimental.pallas import tpu as pltpu
from jax.sharding import PartitionSpec as P

EPS = 1e-06
LIMIT = 7.0
ALPHA = 1.702


def rms_norm(tokens, norm_gain):
    values = tokens.astype(jnp.float32)
    scale = lax.rsqrt(jnp.mean(values * values, axis=-1, keepdims=True) + EPS)
    return (values * scale * norm_gain).astype(jnp.bfloat16)


def clamped_unit(gate_pre, up_pre):
    gate = jnp.minimum(gate_pre, LIMIT)
    up_part = jnp.clip(up_pre, -LIMIT, LIMIT)
    return ((up_part + 1.0) * gate * jax.nn.sigmoid(ALPHA * gate)).astype(jnp.bfloat16)


def slot_numbers(id_blocks, experts, capacity):
    onehot = (id_blocks[:, :, None] == jnp.arange(experts, dtype=jnp.int32)[None, None, :]).astype(
        jnp.int32
    )
    before = jnp.cumsum(onehot, axis=1) - onehot
    position = jnp.sum(before * onehot, axis=2)
    return id_blocks * capacity + position


def project_down(hidden, down_weight):
    result = jnp.einsum(
        "sejf,efd->sejd",
        lax.all_gather(hidden, "tp", axis=3, tiled=True),
        down_weight,
        preferred_element_type=jnp.float32,
    )
    return result.astype(jnp.bfloat16)


def plain_path(tokens, expert_ids, route_weight, norm_gain, gate_weight, up_weight, down_weight):
    n_ep = lax.axis_size("ep")
    n_tp = lax.axis_size("tp")
    tok_rows, width = tokens.shape
    top = expert_ids.shape[1]
    local_experts = gate_weight.shape[0]
    experts = local_experts * n_ep
    capacity = 5 * tok_rows * top // (4 * experts)
    cols = width // n_tp
    normed = rms_norm(tokens, norm_gain)
    dest = slot_numbers(expert_ids.reshape(1, tok_rows * top), experts, capacity).reshape(-1)
    slot_range = jnp.arange(experts * capacity, dtype=jnp.int32)
    match = slot_range[:, None] == dest[None, :]
    pick = jnp.any(match.reshape(experts * capacity, tok_rows, top), axis=2).astype(jnp.bfloat16)
    own = lax.dynamic_slice_in_dim(normed, lax.axis_index("tp") * cols, cols, 1)
    buffer = jnp.dot(pick, own, preferred_element_type=jnp.float32).astype(jnp.bfloat16)
    buffer = buffer.reshape(n_ep, local_experts, capacity, cols)
    arrived = lax.all_to_all(buffer, "ep", split_axis=0, concat_axis=0, tiled=True)
    piece = lax.all_gather(arrived, "tp", axis=3, tiled=True)
    gate_part = jnp.einsum("sejd,edf->sejf", piece, gate_weight, preferred_element_type=jnp.float32)
    up_part = jnp.einsum("sejd,edf->sejf", piece, up_weight, preferred_element_type=jnp.float32)
    hidden = clamped_unit(gate_part, up_part)
    result = project_down(hidden, down_weight)
    back = lax.all_to_all(result, "ep", split_axis=0, concat_axis=0, tiled=True).reshape(
        experts * capacity, cols
    )
    chosen = jnp.transpose(match).astype(jnp.bfloat16)
    per_copy = jnp.dot(chosen, back, preferred_element_type=jnp.float32).reshape(
        tok_rows, top, cols
    )
    mixed = jnp.sum(per_copy * route_weight[:, :, None], axis=1)
    return mixed.astype(jnp.bfloat16)


VMEM_BYTES = 47 * 1024 * 1024
COLUMN_TILE = 256
PIECES = 2


def flip(value, bits):
    bit = 1
    while bit <= bits:
        if bits & bit:
            value = value + bit - 2 * bit * lax.rem(lax.div(value, jnp.int32(bit)), jnp.int32(2))
        bit *= 2
    return value


def fused_kernel(
    n_ep,
    n_tp,
    capacity,
    slots,
    tokens_hbm,
    ids_row_hbm,
    route_row_hbm,
    gain_hbm,
    gate_hbm,
    up_hbm,
    down_hbm,
    out_ref,
    tokens_ref,
    ids_row_ref,
    route_row_ref,
    gain_ref,
    gate_v,
    up_v,
    down_v,
    scales,
    normed,
    outbox,
    outedge,
    fullbox,
    fulledge,
    zedge,
    pairedge,
    xbuf,
    hbuf,
    obuf,
    obedge,
    back,
    backedge,
    acc,
    mixed,
    small_sem,
    weight_sem,
    z_send,
    z_recv,
    pair_send,
    pair_recv,
    g_send,
    g_recv,
    b_send,
    b_recv,
):
    pairs = n_ep // 2
    rows = 2 * capacity
    lead = slots - capacity
    second = rows - slots
    tok_rows, width = tokens_ref.shape
    cols = xbuf.shape[-1]
    hid = hbuf.shape[-1]
    outs = obuf.shape[-1]
    ep = lax.axis_index("ep")
    tp = lax.axis_index("tp")
    pair = lax.div(ep, jnp.int32(2))
    core = lax.rem(ep, jnp.int32(2))
    side = (flip(tp, 1), flip(tp, 2))
    far = flip(tp, 3)
    inner = lax.rem(pair + lax.div(pair, jnp.int32(2)), jnp.int32(2))
    chip_of = [flip(pair, k) for k in range(pairs)]

    top, low = pl.ds(0, tok_rows // 2), pl.ds(tok_rows // 2, tok_rows // 2)
    small = (
        (ids_row_hbm, ids_row_ref),
        (gain_hbm, gain_ref),
        (tokens_hbm.at[top], tokens_ref.at[top]),
        (tokens_hbm.at[low], tokens_ref.at[low]),
        (route_row_hbm, route_row_ref),
    )
    small_loads = [
        pltpu.make_async_copy(a, b, small_sem.at[i]) for i, (a, b) in enumerate(small)
    ]
    for load in small_loads:
        load.start()
    half_hid = hid // 2
    parts = [
        (hbm.at[0, :, lanes], vmem.at[:, lanes])
        for lanes in (pl.ds(0, half_hid), pl.ds(half_hid, half_hid))
        for hbm, vmem in ((gate_hbm, gate_v), (up_hbm, up_v))
    ]
    parts.append((down_hbm.at[0], down_v))
    loads = [pltpu.make_async_copy(a, b, weight_sem.at[i]) for i, (a, b) in enumerate(parts)]

    barrier = pltpu.get_barrier_semaphore()
    for k in range(1, n_ep):
        pl.semaphore_signal(
            barrier, inc=1, device_id=(flip(ep, k), tp), device_id_type=pl.DeviceIdType.MESH
        )
    for other in side:
        pl.semaphore_signal(
            barrier, inc=1, device_id=(ep, other), device_id_type=pl.DeviceIdType.MESH
        )

    own_cols = pl.ds(pl.multiple_of(tp * cols, cols), cols)
    far_cols = pl.ds(pl.multiple_of(far * cols, cols), cols)

    def scale_rows(i, carry):
        at = pl.ds(pl.multiple_of(i * 32, 32), 32)
        values = tokens_ref[at, :].astype(jnp.float32)
        scale = lax.rsqrt(jnp.mean(values * values, axis=-1, keepdims=True) + EPS)
        scales[at, :] = jnp.broadcast_to(scale, (32, scales.shape[1]))
        for where in (own_cols, far_cols):
            values = tokens_ref[at, where].astype(jnp.float32)
            normed[at, where] = (values * scale * gain_ref[:, where]).astype(jnp.bfloat16)
        return carry

    with jax.named_scope("small_wait"):
        small_loads[0].wait()

    ids_row = ids_row_ref[...]
    expert_col = lax.broadcasted_iota(jnp.int32, (n_ep, tok_rows), 0)
    hits_row = ((ids_row[0:1, :] == expert_col) | (ids_row[1:2, :] == expert_col)).astype(
        jnp.float32
    ).astype(jnp.bfloat16)
    first = lax.broadcasted_iota(jnp.int32, (tok_rows, tok_rows), 0)
    second_at = lax.broadcasted_iota(jnp.int32, (tok_rows, tok_rows), 1)
    earlier = (first < second_at).astype(jnp.float32).astype(jnp.bfloat16)
    before_row = jnp.dot(hits_row, earlier, preferred_element_type=jnp.float32)
    slot_row = [
        jnp.sum(jnp.where(ids_row[k : k + 1, :] == expert_col, before_row, 0.0), axis=0, keepdims=True)
        for k in range(2)
    ]
    block_row = lax.broadcasted_iota(jnp.int32, (slots, tok_rows), 0)
    edge_slot = second * (1 - core) - second

    def slots_at(shift):
        edge_row = block_row - shift
        at = jnp.where(
            block_row < second,
            block_row + lead * core,
            jnp.where((edge_row >= second) & (edge_row < capacity), edge_row + edge_slot, -1),
        )
        return at.astype(jnp.float32)

    slot_at = slots_at(0)

    def pick_of(expert):
        taken = ((ids_row[0:1, :] == expert) & (slot_row[0] == slot_at)) | (
            (ids_row[1:2, :] == expert) & (slot_row[1] == slot_at)
        )
        return taken.astype(jnp.float32).astype(jnp.bfloat16)

    def picked(pick, where):
        return jnp.dot(pick, normed[:, where], preferred_element_type=jnp.float32)

    with jax.named_scope("wait_top"):
        small_loads[1].wait()
        small_loads[2].wait()
    steps = tok_rows // 64
    with jax.named_scope("scale_top"):
        lax.fori_loop(0, steps, scale_rows, 0)
    with jax.named_scope("wait_low"):
        small_loads[3].wait()
        small_loads[4].wait()
    for load in loads:
        load.start()
    with jax.named_scope("scale_low"):
        lax.fori_loop(steps, 2 * steps, scale_rows, 0)

    box_cols = (tp, tp, tp, far) + side + (far,)

    def box_flip(box):
        return {0: 2, 1: 3, 6: 3}.get(box, 1)

    def mains(at):
        return pl.ds(pl.multiple_of(slots * at, 8), second)

    def z_copies(box, c):
        for src, dst in (
            (outbox.at[box, c], xbuf.at[box_flip(box), box_cols[box], mains(core)]),
            (outedge.at[box, c], zedge.at[box, core]),
        ):
            yield pltpu.make_async_remote_copy(
                src_ref=src,
                dst_ref=dst,
                send_sem=z_send.at[box // 4],
                recv_sem=z_recv.at[(0, 1, 2, 2, 3, 5, 4)[box]],
                device_id=(flip(pair, box_flip(box)) * 2 + c, tp),
                device_id_type=pl.DeviceIdType.MESH,
            )

    def bytes_of(ref, send, recv):
        return pltpu.make_async_remote_copy(
            src_ref=ref,
            dst_ref=ref,
            send_sem=send,
            recv_sem=recv,
            device_id=(ep, side[0]),
            device_id_type=pl.DeviceIdType.MESH,
        )

    def z_wait(at, ref):
        bytes_of(ref, z_send.at[0], z_recv.at[at]).wait_recv()

    def fold(values):
        return jnp.concatenate([values[:, : cols // 2], values[:, cols // 2 :]], axis=0)

    def z_fill(box):
        where = pl.ds(pl.multiple_of(box_cols[box] * cols, cols), cols)
        for c in range(2):
            values = picked(pick_of(flip(pair, box_flip(box)) * 2 + c), where)
            outbox[box, c] = values[:second].astype(jnp.bfloat16)
            outedge[box, c] = fold(values[second:capacity]).astype(jnp.bfloat16)

    def z_start(box, cs=(0, 1)):
        for c in cs:
            for copy in z_copies(box, c):
                copy.start()

    def z_sends(boxes_in_order):
        for box in boxes_in_order:
            z_fill(box)
            z_start(box)

    def norm_rest(i, carry):
        at = pl.ds(pl.multiple_of(i * 32, 32), 32)
        for other in side:
            where = pl.ds(pl.multiple_of(other * cols, cols), cols)
            values = tokens_ref[at, where].astype(jnp.float32)
            normed[at, where] = (values * scales[at, 0:1] * gain_ref[:, where]).astype(
                jnp.bfloat16
            )
        return carry

    partner = flip(ep, 1)

    def pair_copies():
        for src, dst in (
            (fullbox, xbuf.at[0, :, mains(core)]),
            (fulledge, pairedge.at[core]),
        ):
            yield pltpu.make_async_remote_copy(
                src_ref=src,
                dst_ref=dst,
                send_sem=pair_send,
                recv_sem=pair_recv,
                device_id=(partner, tp),
                device_id_type=pl.DeviceIdType.MESH,
            )

    def pair_fill():
        lax.fori_loop(0, tok_rows // 32, norm_rest, 0)
        theirs = pick_of(partner)
        for j in range(n_tp):
            values = picked(theirs, slice(j * cols, (j + 1) * cols))
            fullbox[j] = values[:second].astype(jnp.bfloat16)
            fulledge[j] = fold(values[second:capacity]).astype(jnp.bfloat16)

    def outer_fill():
        z_fill(2)
        z_fill(0)

    def outer_sends():
        for c in range(2):
            z_start(2, (c,))
            z_start(0, (c,))
        pair_fill()

    def inner_sends():
        z_start(0)
        z_sends((2,))
        pair_fill()

    with jax.named_scope("fill"):
        pl.when(inner == 1)(lambda: z_fill(0))
        pl.when(inner == 0)(outer_fill)
    with jax.named_scope("barrier"):
        pl.semaphore_wait(barrier, n_ep - 1 + 2)
    with jax.named_scope("z_sends"):
        pl.when(inner == 1)(inner_sends)
        pl.when(inner == 0)(outer_sends)
    with jax.named_scope("pair_pick"):
        for copy in pair_copies():
            copy.start()
        mine = pick_of(ep)
        for j in range(n_tp):
            values = picked(mine, slice(j * cols, (j + 1) * cols))
            xbuf[0, j, mains(core), :] = values[:second].astype(jnp.bfloat16)
            pairedge[core, j] = fold(values[second:capacity]).astype(jnp.bfloat16)
        pl.when(inner == 1)(lambda: z_sends((1,)))
        pl.when(inner == 0)(lambda: z_sends((3, 1)))

    def join(k, j, low, high):
        for half in range(2):
            mid = [v[lead * half : lead * half + lead, :] for v in (low, high)]
            lanes = slice(half * (cols // 2), (half + 1) * (cols // 2))
            xbuf[k, j, second:slots, lanes] = jnp.concatenate(mid, axis=0)

    boxes = (xbuf, hbuf)
    half_cols = cols // 2
    spans = {0: (0, slots), 1: (slots, rows), None: (0, rows)}
    both = (0, 1)

    def group(b, k, r):
        return k - 2 if b == 0 else 2 + 2 * k + (r or 0)

    def g_copy(b, k, j, half, r, to, kind):
        start, stop = spans[r]
        where = boxes[b].at[k, j, pl.ds(start, stop - start), pl.ds(half * half_cols, half_cols)]
        return pltpu.make_async_remote_copy(
            src_ref=where,
            dst_ref=where,
            send_sem=g_send.at[b, k],
            recv_sem=g_recv.at[group(b, k, r), kind],
            device_id=(ep, to),
            device_id_type=pl.DeviceIdType.MESH,
        )

    def block_copy(b, k, d, half, r):
        return g_copy(b, k, tp, half, r, side[d], d if half == d else 2)

    def take(b, k, r=None):
        for d in range(2):
            with jax.named_scope(f"w_relay_{b}_{r}"):
                g_copy(b, k, side[d], d, r, side[d], d).wait_recv()

    def hand(b, k, r=None):
        for d in range(2):
            g_copy(b, k, side[d], d, r, side[1 - d], 3).start()

    def relay(b, k, r=None):
        for d in range(2):
            with jax.named_scope(f"w_relay_{b}_{r}"):
                g_copy(b, k, side[d], d, r, side[d], d).wait_recv()
            g_copy(b, k, side[d], d, r, side[1 - d], 3).start()

    def arrive(b, k, r, kind):
        start, stop = spans[r]
        where = boxes[b].at[k, far, pl.ds(start, stop - start), :]
        bytes_of(where, g_send.at[b, k], g_recv.at[group(b, k, r), kind]).wait_recv()

    def send_half(b, k, half, r=None):
        for d in range(2):
            block_copy(b, k, d, half, r).start()

    def send_first(b, k, r=None):
        for d in range(2):
            block_copy(b, k, d, d, r).start()

    def send_rest(b, k, r=None):
        for d in range(2):
            block_copy(b, k, d, 1 - d, r).start()

    def spread(b, k, r=None):
        send_first(b, k, r)
        send_rest(b, k, r)

    def near(b, k, r=None):
        with jax.named_scope(f"w_near_{b}_{r}"):
            arrive(b, k, r, 2)

    def distant(b, k, r=None):
        with jax.named_scope(f"w_far_{b}_{r}"):
            arrive(b, k, r, 3)

    def enter(k):
        with jax.named_scope("w_z"):
            z_wait(k - 2, xbuf.at[k, tp])
        join(k, tp, zedge[k - 2, 0], zedge[k - 2, 1])

    def enter_far():
        with jax.named_scope("w_zfar"):
            z_wait(4, xbuf.at[3, far])
        join(3, far, zedge[6, 0], zedge[6, 1])

    def enter_next(part):
        first_box, count, at = ((2, 2, 2), (4, 1, 3), (5, 1, 5))[part]
        with jax.named_scope(f"w_z1_{part}"):
            z_wait(at, xbuf.at[1, pl.ds(0, count)])
        for box in range(first_box, first_box + count):
            join(1, box_cols[box], zedge[box, 0], zedge[box, 1])

    def dot_blocks(box, k, r, weight, where, blocks):
        depth = box.shape[-1]
        start, stop = spans[r]
        total = None
        for j, half in blocks:
            size = depth if half is None else depth // 2
            at = j * depth if isinstance(j, int) else pl.multiple_of(j * depth, depth)
            at = at + (half or 0) * size
            lanes = slice((half or 0) * size, (half or 0) * size + size)
            part = jnp.dot(
                box[k, j, start:stop, lanes], weight[pl.ds(at, size), where],
                preferred_element_type=jnp.float32,
            )
            total = part if total is None else total + part
        return total

    every = tuple((j, None) for j in range(n_tp))
    sides = tuple((j, None) for j in side)
    close = ((tp, None),) + sides

    def column(i):
        return pl.ds(pl.multiple_of(i * COLUMN_TILE, COLUMN_TILE), COLUMN_TILE)

    stages = {
        None: (every, None, None),
        "near": (close, None, 0),
        "far": (((far, None),), 0, None),
        "own": (((tp, None), (far, None)), None, 2),
        "third": (sides[:1], 2, 2),
        "fourth": (sides[1:], 2, None),
        "mine": (close[:1], None, 0),
        "sides": (sides, 0, 0),
        "own_last": (((tp, None), (far, None), (side[0], 0), (side[1], 1)), None, 0),
        "side_last": (((side[0], 1), (side[1], 0)), 0, None),
    }

    def units(k, stage=None, halves=both):
        blocks, start, keep = stages[stage]

        def tile(i, carry):
            where = column(i)
            gate_pre = dot_blocks(xbuf, k, None, gate_v, where, blocks)
            up_pre = dot_blocks(xbuf, k, None, up_v, where, blocks)
            if start is not None:
                gate_pre = gate_pre + acc[start, :, where]
                up_pre = up_pre + acc[start + 1, :, where]
            if keep is not None:
                acc[keep, :, where] = gate_pre
                acc[keep + 1, :, where] = up_pre
            else:
                hbuf[k, tp, :, where] = clamped_unit(gate_pre, up_pre)
            return carry

        tiles = hid // COLUMN_TILE // 2
        with jax.named_scope(f"units_{stage}"):
            lax.fori_loop(halves[0] * tiles, (halves[-1] + 1) * tiles, tile, 0)

    def produce(k, stage, r=None):
        for half in both:
            units(k, stage, (half,))
            block_copy(1, k, half, half, r).start()
        send_rest(1, k, r)

    piece = outs // PIECES

    def back_copy(src, dst, to, group_at):
        return pltpu.make_async_remote_copy(
            src_ref=src,
            dst_ref=dst,
            send_sem=b_send.at[group_at // 2],
            recv_sem=b_recv.at[group_at],
            device_id=(to, tp),
            device_id_type=pl.DeviceIdType.MESH,
        )

    def back_send(k, c, to, at, group_at):
        lanes = pl.ds(at * piece, piece)
        back_copy(obuf.at[k, mains(c), lanes], back.at[ep, :, lanes], to, group_at).start()
        if at == PIECES - 1:
            back_copy(obedge.at[k, c], backedge.at[ep], to, group_at).start()

    def results(name, stage, r=None):
        k = name
        start, stop = spans[r]
        blocks, begun, keep = stages[stage]
        at_acc = {0: 5, 1: 2}.get(name, 4)

        def tile(i, carry):
            where = column(i)
            total = dot_blocks(hbuf, k, r, down_v, where, blocks)
            if begun is not None:
                total = total + acc[at_acc, start:stop, where]
            if keep is not None:
                acc[at_acc, start:stop, where] = total
                return carry
            obuf[k, start:stop, where] = total.astype(jnp.bfloat16)
            return carry

        tiles = outs // COLUMN_TILE // PIECES
        for at in range(PIECES):
            with jax.named_scope(f"results_{name}_{stage}_{r}"):
                lax.fori_loop(at * tiles, (at + 1) * tiles, tile, 0)
            if keep is not None:
                continue
            if at == PIECES - 1 and r != 1:
                mid = obuf[k, second:slots, :].astype(jnp.float32)
                for c in both:
                    obedge[k, c] = fold(mid[lead * c : lead * c + lead]).astype(jnp.bfloat16)
            if name == 0:
                back_send(0, 1 - core, partner, at, 2)
            else:
                for c in both if r is None else (r,):
                    back_send(k, c, chip_of[name] * 2 + c, at, int(name == 1))
        if name == 0 and keep is None:
            back[ep] = obuf[0, mains(core), :]
            backedge[ep] = obedge[0, core]

    def begin(name, r=None):
        near(1, name, r)
        results(name, "near" if r is None else "sides", r)

    def finish(name, r=None):
        distant(1, name, r)
        results(name, "far", r)

    mixed_chips = ((pair, chip_of[2], chip_of[3]), (chip_of[1],))

    def share_of(part, at_slots):
        shares = []
        for chip in mixed_chips[part]:
            for c in both:
                share = None
                for k in range(2):
                    hit = (ids_row[k : k + 1, :] == chip * 2 + c) & (slot_row[k] == at_slots)
                    one = jnp.where(hit, route_row_ref[k : k + 1, :], 0.0)
                    share = one if share is None else share + one
                shares.append(share)
        share = jnp.transpose(jnp.concatenate(shares, axis=0))
        high = share.astype(jnp.bfloat16)
        low = (share - high.astype(jnp.float32)).astype(jnp.bfloat16)
        return jnp.concatenate([high, low], axis=1)

    def mix(part):
        shares = [share_of(part, at_slots) for at_slots in (slot_at, slots_at(lead))]
        with jax.named_scope(f"w_back_{part}"):
            if part == 0:
                half = obuf.at[0, :, pl.ds(0, outs // 2)]
                bytes_of(half, b_send.at[1], b_recv.at[2]).wait_recv()
            got = xbuf.at[0, pl.ds(0, 1 if part else 2)]
            bytes_of(got, b_send.at[0], b_recv.at[part]).wait_recv()
        with jax.named_scope(f"mix_{part}"):
            for i in range(outs // COLUMN_TILE):
                where = slice(i * COLUMN_TILE, (i + 1) * COLUMN_TILE)
                half = i * COLUMN_TILE // (outs // 2)
                lanes = slice(where.start - half * (outs // 2), where.stop - half * (outs // 2))
                blocks = []
                for chip in mixed_chips[part]:
                    for c in both:
                        blocks += [back[chip * 2 + c, :, where], backedge[chip * 2 + c, :, lanes]]
                table = jnp.concatenate(blocks + blocks, axis=0)
                total = jnp.dot(shares[half], table, preferred_element_type=jnp.float32)
                if part == 0:
                    mixed[:, where] = total
                else:
                    out_ref[:, where] = (mixed[:, where] + total).astype(jnp.bfloat16)

    def sends_done():
        with jax.named_scope("w_sends"):
            bytes_of(xbuf.at[0], z_send.at[0], z_recv.at[0]).wait_send()
            bytes_of(xbuf.at[0, pl.ds(0, 3)], z_send.at[1], z_recv.at[0]).wait_send()
            bytes_of(xbuf.at[0, pl.ds(0, 2)], pair_send, z_recv.at[0]).wait_send()
            half = obuf.at[0, :, pl.ds(0, outs // 2)]
            bytes_of(half, b_send.at[1], b_recv.at[2]).wait_send()
            for b in range(2):
                for k in range(2 - 2 * b, pairs):
                    if (b, k) != (1, 1):
                        sent = boxes[b].at[k, pl.ds(0, 2 if (b, k) == (0, 3) else 3)]
                        bytes_of(sent, g_send.at[b, k], g_recv.at[0, 0]).wait_send()

    with jax.named_scope("w_pair"):
        bytes_of(xbuf.at[0, pl.ds(0, 2)], pair_send, pair_recv).wait_recv()
    for j in range(n_tp):
        join(0, j, pairedge[0, j], pairedge[1, j])
    with jax.named_scope("w_gateup"):
        loads[0].wait()
        loads[1].wait()
    units(0, None, (0,))
    send_half(1, 0, 0)
    pl.when(inner == 1)(lambda: z_sends((3, 6)))
    with jax.named_scope("w_gateup"):
        loads[2].wait()
        loads[3].wait()
    units(0, None, (1,))

    def outer_order():
        z_sends((6, 4, 5))
        enter(2)
        spread(0, 2)
        relay(0, 2)
        near(0, 2)
        send_half(1, 0, 1)
        units(2, "near")
        distant(0, 2)
        produce(2, "far")
        enter_next(0)
        units(1, "own")
        loads[4].wait()
        take(1, 0)
        begin(0)
        relay(1, 2)
        enter(3)
        spread(0, 3)
        begin(2)
        finish(2)
        hand(1, 0)
        enter_far()
        take(0, 3)
        units(3, "own_last")
        near(0, 3)
        produce(3, "side_last", 0)
        send_first(1, 3, 1)
        finish(0)
        results(3, "mine")
        relay(1, 3, 0)
        send_rest(1, 3, 1)
        enter_next(1)
        units(1, "third")
        relay(1, 3, 1)
        enter_next(2)
        produce(1, "fourth", 0)
        send_first(1, 1, 1)
        begin(3, 0)
        finish(3, 0)
        begin(3, 1)
        relay(1, 1, 0)
        send_rest(1, 1, 1)
        finish(3, 1)
        results(1, "mine")
        relay(1, 1, 1)
        begin(1, 0)
        sends_done()
        finish(1, 0)
        begin(1, 1)
        finish(1, 1)
        mix(0)

    def inner_order():
        send_half(1, 0, 1)
        z_sends((4, 5))
        enter(2)
        spread(0, 2)
        relay(0, 2)
        near(0, 2)
        units(2, "near")
        enter(3)
        send_first(0, 3)
        distant(0, 2)
        produce(2, "far")
        enter_next(0)
        units(1, "own")
        loads[4].wait()
        take(1, 0)
        begin(0)
        relay(1, 2)
        send_rest(0, 3)
        begin(2)
        finish(2)
        hand(1, 0)
        enter_far()
        take(0, 3)
        units(3, "own_last")
        near(0, 3)
        produce(3, "side_last", 0)
        send_first(1, 3, 1)
        finish(0)
        results(3, "mine")
        relay(1, 3, 0)
        send_rest(1, 3, 1)
        enter_next(1)
        units(1, "third")
        enter_next(2)
        units(1, "fourth")
        relay(1, 3, 1)
        spread(1, 1, 0)
        send_first(1, 1, 1)
        begin(3, 0)
        finish(3, 0)
        begin(3, 1)
        relay(1, 1, 0)
        send_rest(1, 1, 1)
        finish(3, 1)
        results(1, "mine")
        relay(1, 1, 1)
        begin(1, 0)
        sends_done()
        finish(1, 0)
        begin(1, 1)
        finish(1, 1)
        mix(0)

    pl.when(inner == 0)(outer_order)
    pl.when(inner == 1)(inner_order)

    with jax.named_scope("w_sends_2"):
        bytes_of(boxes[1].at[1, pl.ds(0, 3)], g_send.at[1, 1], g_recv.at[0, 0]).wait_send()
        bytes_of(xbuf.at[0, pl.ds(0, 3)], b_send.at[0], b_recv.at[0]).wait_send()
    mix(1)


def fused_path(
    n_ep, n_tp, tokens, expert_ids, route_weight, norm_gain, gate_weight, up_weight, down_weight
):
    tok_rows, width = tokens.shape
    capacity, slots = slots_of(n_ep, tokens.shape, expert_ids.shape)
    rows = 2 * capacity
    main, edge = rows - slots, 2 * (slots - capacity)
    hid = gate_weight.shape[2]
    outs = down_weight.shape[2]
    cols = width // n_tp
    pairs = n_ep // 2
    vmem = pl.BlockSpec(memory_space=pltpu.VMEM)
    hbm = pl.BlockSpec(memory_space=pltpu.HBM)
    dma = pltpu.SemaphoreType.DMA
    arrays = (
        tokens,
        jnp.transpose(expert_ids),
        jnp.transpose(route_weight),
        norm_gain.reshape(1, width),
        gate_weight,
        up_weight,
        down_weight,
    )
    return pl.pallas_call(
        functools.partial(fused_kernel, n_ep, n_tp, capacity, slots),
        out_shape=jax.ShapeDtypeStruct((tok_rows, outs), jnp.bfloat16),
        in_specs=[hbm] * 7,
        out_specs=vmem,
        scratch_shapes=[
            pltpu.VMEM(tokens.shape, tokens.dtype),
            pltpu.VMEM(expert_ids.shape[::-1], expert_ids.dtype),
            pltpu.VMEM(route_weight.shape[::-1], route_weight.dtype),
            pltpu.VMEM((1, width), norm_gain.dtype),
            pltpu.VMEM(gate_weight.shape[1:], jnp.bfloat16),
            pltpu.VMEM(up_weight.shape[1:], jnp.bfloat16),
            pltpu.VMEM(down_weight.shape[1:], jnp.bfloat16),
            pltpu.VMEM((tok_rows, 128), jnp.float32),
            pltpu.VMEM((tok_rows, width), jnp.bfloat16),
            pltpu.VMEM((pairs + 3, 2, main, cols), jnp.bfloat16),
            pltpu.VMEM((pairs + 3, 2, edge, cols // 2), jnp.bfloat16),
            pltpu.VMEM((n_tp, main, cols), jnp.bfloat16),
            pltpu.VMEM((n_tp, edge, cols // 2), jnp.bfloat16),
            pltpu.VMEM((pairs + 3, 2, edge, cols // 2), jnp.bfloat16),
            pltpu.VMEM((2, n_tp, edge, cols // 2), jnp.bfloat16),
            pltpu.VMEM((pairs, n_tp, rows, cols), jnp.bfloat16),
            pltpu.VMEM((pairs, n_tp, rows, hid), jnp.bfloat16),
            pltpu.VMEM((pairs, rows, outs), jnp.bfloat16),
            pltpu.VMEM((pairs, 2, edge, outs // 2), jnp.bfloat16),
            pltpu.VMEM((n_ep, main, outs), jnp.bfloat16),
            pltpu.VMEM((n_ep, edge, outs // 2), jnp.bfloat16),
            pltpu.VMEM((6, rows, hid), jnp.float32),
            pltpu.VMEM((tok_rows, outs), jnp.float32),
            dma((5,)),
            dma((5,)),
            dma((2,)),
            dma((6,)),
            dma,
            dma,
            dma((2, pairs)),
            dma((2 + 2 * pairs, 4)),
            dma((2,)),
            dma((3,)),
        ],
        compiler_params=pltpu.CompilerParams(
            collective_id=0, has_side_effects=True, vmem_limit_bytes=VMEM_BYTES
        ),
    )(*(pltpu.with_memory_space_constraint(array, pltpu.HBM) for array in arrays))


def slots_of(n_ep, token_shape, id_shape):
    capacity = 5 * token_shape[0] * id_shape[1] // (4 * n_ep)
    return capacity, -(-capacity // 8) * 8


def on_device(tokens, expert_ids, route_weight, norm_gain, gate_weight, up_weight, down_weight):
    n_ep = lax.axis_size("ep")
    n_tp = lax.axis_size("tp")
    args = (tokens, expert_ids, route_weight, norm_gain, gate_weight, up_weight, down_weight)
    fits = n_tp == 4 and n_ep == 8 and gate_weight.shape[0] == 1 and expert_ids.shape[1] == 2
    capacity, slots = slots_of(n_ep, tokens.shape, expert_ids.shape)
    cols = tokens.shape[1] // n_tp
    even = gate_weight.shape[2] == cols and down_weight.shape[2] == cols
    if fits and even and capacity % 4 == 0 and slots - capacity == 4:
        return fused_path(n_ep, n_tp, *args)
    return plain_path(*args)


def solution(mesh):
    placed = (
        P("ep", None),
        P("ep", None),
        P("ep", None),
        P(),
        P("ep", None, "tp"),
        P("ep", None, "tp"),
        P("ep", None, "tp"),
    )
    return jax.shard_map(
        on_device, mesh=mesh, in_specs=placed, out_specs=P("ep", "tp"), check_vma=False
    )
```
